32 devices in a mesh: sp: 8 (over z, x), tp: 4 (over y, core).
Axes of the slice: x: 2, y: 2, z: 4, core: 2. Of those that a mesh axis runs over, the one named last changes fastest.
Arguments:
- inputs: bfloat16 [4096, 2048], P(('sp', 'tp')), may hold values from -6 to 6
- norm_gain: float32 [2048], replicated, may hold values from 0.1 to 1.9
- w_query: bfloat16 [2048, 1024], P(None, 'tp'), may hold values from -1 to 1
- w_key: bfloat16 [2048, 1024], P(None, 'tp'), may hold values from -1 to 1
- w_value: bfloat16 [2048, 1024], P(None, 'tp'), may hold values from -0.125 to 0.125
- query_gain: float32 [2, 64], replicated, may hold values from 1 to 5.5
- key_gain: float32 [2, 64], replicated, may hold values from 1 to 5.5
- lambdas: float32 [8], P('tp'), may hold values from 0.3 to 0.8
- sub_gain: float32 [128], replicated, may hold values from 0.1 to 1.9
- w_gate_b: bfloat16 [2048, 1024], P(None, 'tp'), may hold values from -0.125 to 0.125
- w_gate_c: bfloat16 [2048, 1024], P(None, 'tp'), may hold values from -0.125 to 0.125
- w_conv_in: bfloat16 [2048, 1024], P(None, 'tp'), may hold values from -0.125 to 0.125
- conv_taps: float32 [3, 1024], P(None, 'tp'), may hold values from -3 to 3
- conv_gain: float32 [1024], P('tp'), may hold values from 0.1 to 1.9
- w_out_att: bfloat16 [1024, 2048], P('tp'), may hold values from -0.125 to 0.125
- w_out_conv: bfloat16 [1024, 2048], P('tp'), may hold values from -0.125 to 0.125
Outputs:
- mixed: float32 [4096, 2048], P(('sp', 'tp'))
- log_sums: float32 [8, 2, 4096], P('tp', None, 'sp')
The draws below stay inside these ranges and needn't reach their ends.
All inputs are finite; a program needn't handle non-finite values.
Results may differ from the reference program's by a relative error of at most 0.034.
Values may be sent and summed in bfloat16 or wider, within the bound.
A program may use at most 192 MiB of HBM per device.

```python
import math
import jax
import jax.numpy as jnp
from jax import lax

D = 2048
ATT_HEADS = 8
QK = 64
VD = 128
CONV = 1024
GROUP = 64
KW = 3
TOKENS = 4096


def draw_query_gain(key, part):
    spread = jax.random.uniform(jax.random.fold_in(key, 11), (2, QK), jnp.float32, -1.0, 1.0)
    return 1.3 * (1.0 + 0.2 * spread)


def draw_key_gain(key, part):
    spread = jax.random.uniform(jax.random.fold_in(key, 23), (2, QK), jnp.float32, -1.0, 1.0)
    return 1.3 * (1.0 + 0.2 * spread)


def projection_pair(key):
    first = jax.random.normal(jax.random.fold_in(key, 101), (D, ATT_HEADS * 2 * QK), jnp.float32)
    second = jax.random.normal(jax.random.fold_in(key, 103), (D, ATT_HEADS * 2 * QK), jnp.float32)
    scale = D ** (-0.5)
    return (jnp.clip(first, -5.0, 5.0) * scale, jnp.clip(second, -5.0, 5.0) * scale)


def draw_w_query(key, part):
    first, second = projection_pair(key)
    return first.astype(jnp.bfloat16)


def draw_w_key(key, part):
    first, second = projection_pair(key)
    return second.astype(jnp.bfloat16)


def draw_inputs(key, part):
    base = jax.random.normal(jax.random.fold_in(key, 201), (TOKENS, D), jnp.float32)
    return jnp.clip(base, -6.0, 6.0).astype(jnp.bfloat16)


def block_levels(own_key, shape, pieces, low, high):
    loudness = 1.0
    for dim, shards_of in pieces:
        draws = jax.random.uniform(jax.random.fold_in(jax.random.fold_in(own_key, 6), dim), (shards_of,), jnp.float32, low / len(pieces), high / len(pieces))
        loudness = loudness * jnp.repeat(jnp.exp(draws), shape[dim] // shards_of).reshape((-1,) + (1,) * (len(shape) - 1 - dim))
    return loudness


def scatter_about(key, shape, deviation, reach, cuts=(), held_as=jnp.bfloat16):
    array = jax.random.normal(key, shape, jnp.float32) * deviation
    if len(cuts) > 0:
        array = block_levels(key, shape, cuts, -0.22, 0.18) * array
    return jnp.clip(array, min=-reach, max=reach).astype(held_as)


def setup_inputs(seed: int = 0) -> dict:
    key_list = jax.random.split(jax.random.key(seed), 17)
    inputs = draw_inputs(jax.random.fold_in(key_list[16], 71), 0)
    norm_gain = jnp.clip(1.0 + 0.18 * jax.random.normal(key_list[1], (D,), jnp.float32), 0.1, 1.9)
    w_query = draw_w_query(jax.random.fold_in(key_list[16], 71), 0)
    w_key = draw_w_key(jax.random.fold_in(key_list[16], 71), 0)
    w_value = scatter_about(key_list[4], (D, ATT_HEADS * VD), D ** -0.5, 0.125, ((1, 4),))
    query_gain = draw_query_gain(jax.random.fold_in(key_list[16], 71), 0)
    key_gain = draw_key_gain(jax.random.fold_in(key_list[16], 71), 0)
    lambdas = jnp.clip(0.3 + 0.5 * jax.random.uniform(key_list[7], (ATT_HEADS,), jnp.float32) ** block_levels(key_list[7], (ATT_HEADS,), ((0, 4),), -0.2, 0.2), 0.3, 0.8)
    sub_gain = jnp.clip(1.0 + 0.18 * jax.random.normal(key_list[8], (VD,), jnp.float32), 0.1, 1.9)
    w_gate_b = scatter_about(key_list[9], (D, CONV), D ** -0.5, 0.125, ((1, 4),))
    w_gate_c = scatter_about(key_list[10], (D, CONV), D ** -0.5, 0.125, ((1, 4),))
    w_conv_in = scatter_about(key_list[11], (D, CONV), D ** -0.5, 0.125, ((1, 4),))
    conv_taps = scatter_about(key_list[12], (KW, CONV), 0.577, 3.0, ((1, 4),), jnp.float32)
    conv_gain = jnp.clip(1.0 + 0.18 * jax.random.normal(key_list[13], (CONV,), jnp.float32), 0.1, 1.9)
    w_out_att = scatter_about(key_list[14], (ATT_HEADS * VD, D), (ATT_HEADS * VD + CONV) ** -0.5, 0.125, ((0, 4),))
    w_out_conv = scatter_about(key_list[15], (CONV, D), (ATT_HEADS * VD + CONV) ** -0.5, 0.125, ((0, 4),))
    return {"inputs": inputs, "norm_gain": norm_gain, "w_query": w_query, "w_key": w_key, "w_value": w_value, "query_gain": query_gain, "key_gain": key_gain, "lambdas": lambdas, "sub_gain": sub_gain, "w_gate_b": w_gate_b, "w_gate_c": w_gate_c, "w_conv_in": w_conv_in, "conv_taps": conv_taps, "conv_gain": conv_gain, "w_out_att": w_out_att, "w_out_conv": w_out_conv}


eps = 1e-06

def rms_scale(values):
    return values * lax.rsqrt(lax.optimization_barrier(jnp.mean(values * values, axis=-1, keepdims=True)) + eps)

def rounded(values):
    return lax.optimization_barrier(values.astype(jnp.bfloat16)).astype(jnp.float32)

def reference(inputs, norm_gain, w_query, w_key, w_value, query_gain, key_gain, lambdas, sub_gain, w_gate_b, w_gate_c, w_conv_in, conv_taps, conv_gain, w_out_att, w_out_conv):
    length = inputs.shape[0]
    normed = (rms_scale(inputs.astype(jnp.float32)) * norm_gain).astype(jnp.bfloat16)

    def project(weight):
        return jnp.dot(normed, weight, preferred_element_type=jnp.float32).astype(jnp.bfloat16)
    query = project(w_query).reshape(length, ATT_HEADS, 2, QK)
    key = project(w_key).reshape(length, ATT_HEADS, 2, QK)
    value = project(w_value).reshape(length, ATT_HEADS, VD)
    qn = (rms_scale(query.astype(jnp.float32)) * query_gain * QK ** (-0.5)).astype(jnp.bfloat16)
    kn = (rms_scale(key.astype(jnp.float32)) * key_gain).astype(jnp.bfloat16)
    keys_f = kn.astype(jnp.float32)
    values_f = value.astype(jnp.float32)
    qblock = math.gcd(length, 128)
    key_pos = jnp.arange(length, dtype=jnp.int32)

    def one_block(start):
        qrows = lax.dynamic_slice_in_dim(qn, start, qblock, 0).astype(jnp.float32)
        scores = jnp.einsum('qhmd,khmd->hmqk', qrows, keys_f)
        query_pos = start + jnp.arange(qblock, dtype=jnp.int32)
        allowed = key_pos[None, :] <= query_pos[:, None]
        scores = jnp.where(allowed, scores, -1e+30)
        top = lax.optimization_barrier(jnp.max(scores, axis=-1, keepdims=True))
        prob = jnp.where(allowed, jnp.exp(scores - top), 0.0)
        total = lax.optimization_barrier(jnp.sum(prob, axis=-1))
        acc = jnp.einsum('hmqk,khd->hmqd', rounded(prob), values_f)
        return (acc / total[..., None], top[..., 0] + jnp.log(total))
    starts = (jnp.arange(length // qblock) * qblock).astype(jnp.int32)
    outs, logs = lax.map(one_block, starts)
    map_out = outs.transpose(1, 2, 0, 3, 4).reshape(ATT_HEADS, 2, length, VD)
    attn = map_out[:, 0] - lambdas[:, None, None] * map_out[:, 1]
    heads_out = (rms_scale(attn) * sub_gain).astype(jnp.bfloat16)
    heads_out = heads_out.transpose(1, 0, 2).reshape(length, ATT_HEADS * VD)
    log_sums = logs.transpose(1, 2, 0, 3).reshape(ATT_HEADS, 2, length)
    gate_b = project(w_gate_b).astype(jnp.float32)
    gate_c = project(w_gate_c).astype(jnp.float32)
    conv_in = project(w_conv_in).astype(jnp.float32)
    u_vals = rounded(gate_c * conv_in)
    padded = jnp.concatenate([jnp.zeros((KW - 1, CONV), jnp.float32), u_vals], axis=0)
    conv = jnp.zeros((length, CONV), jnp.float32)
    for tap in range(KW):
        conv = conv + conv_taps[tap] * padded[tap:tap + length]
    gated = gate_b * conv
    grouped = rms_scale(gated.reshape(length, CONV // GROUP, GROUP)).reshape(length, CONV)
    conv_out = (grouped * conv_gain).astype(jnp.bfloat16)
    mixed = jnp.dot(heads_out, w_out_att, preferred_element_type=jnp.float32)
    mixed = mixed + jnp.dot(conv_out, w_out_conv, preferred_element_type=jnp.float32)
    return (mixed, log_sums)
```

```python
import functools

import jax
import jax.numpy as jnp
from jax import lax
from jax.experimental import pallas as pl
from jax.experimental.pallas import tpu as pltpu
from jax.sharding import PartitionSpec as P

GROUP = 64
eps = 1e-06
MESH = pl.DeviceIdType.MESH
VMEM_LIMIT = 62 * 1024 * 1024
CHUNKS = 4
EDGE = 16
TILE = 256


def rms_scale(values):
    return values * lax.rsqrt(jnp.mean(values * values, axis=-1, keepdims=True) + eps)


def flip(index, bit):
    return index + bit - 2 * bit * lax.rem(index // bit, 2)


def remote(src, dst, send, recv, where):
    return pltpu.make_async_remote_copy(
        src_ref=src, dst_ref=dst, send_sem=send, recv_sem=recv, device_id=where,
        device_id_type=MESH,
    )


def group_scale(values, size):
    lanes = values.shape[1]
    row = lax.broadcasted_iota(jnp.int32, (lanes, lanes), 0) // size
    col = lax.broadcasted_iota(jnp.int32, (lanes, lanes), 1) // size
    ones = jnp.where(row == col, 1.0, 0.0).astype(jnp.bfloat16)
    squares = values * values
    high = squares.astype(jnp.bfloat16)
    low = (squares - high.astype(jnp.float32)).astype(jnp.bfloat16)
    sums = jnp.dot(high, ones, preferred_element_type=jnp.float32) + jnp.dot(
        low, ones, preferred_element_type=jnp.float32
    )
    return lax.rsqrt(sums * (1.0 / size) + eps)


def layer(
    sp, tp, comp, heads,
    x_ref, gain_ref, qg_ref, kg_ref, lam_ref, sub_ref, taps_ref, cgain_ref,
    wk, wv, wq, wc, wi, wb, wa, wo,
    out_ref, log_ref,
    held, wbuf, wfull, wobuf, gains, kvb, qb, give_kv, give_q, qpad, top, total, acc, cbuf, tail,
    padded, cvout, cross, fin, far, cross_in, fin_in, far_in, obuf, hin, lout, lin,
    wsem, near_sem, far_send, far_recv, fwd_send, fwd_recv, up_send, kv_recv, gk_send, gq_send,
    q_recv, tail_sem, w_send, w_recv, cross_send, cross_recv, fin_send, fin_recv, fs_send, fs_recv,
    o_send, o_recv, log_sem,
):
    s = lax.axis_index("sp")
    t = lax.axis_index("tp")
    level, side = s // 2, lax.rem(s, 2)
    levels = sp // 2
    mate = level * 2 + 1 - side
    near, away = flip(t, 1), flip(t, 2)
    diag = flip(near, 2)
    first, second = t // 2, 1 - t // 2
    own = x_ref.shape[0]
    rows = own * tp
    half = rows // 2
    head_cols = heads * 2 * comp // 2
    per = heads // 2
    vsize = sub_ref.shape[1]
    both = 2 * comp
    channels = cgain_ref.shape[1]
    has_up, has_down = level < levels - 1, level > 0
    ups, downs = has_up.astype(jnp.int32), has_down.astype(jnp.int32)
    up_id = {"sp": jnp.minimum(s + 2, sp - 2 + side)}
    mate_id = {"sp": mate}

    loads = [
        pltpu.make_async_copy(w, wbuf.at[i], wsem.at[i])
        for i, w in enumerate((wk, wv, wq, wc, wi, wb))
    ]
    for load in loads:
        load.start()
    wa_rows = wa.shape[0]
    half_rows = wa_rows // 2

    def shard(index):
        return pl.ds(pl.multiple_of(index * wa_rows, wa_rows), wa_rows)

    def part_of(index, which):
        return pl.ds(
            pl.multiple_of(index * wa_rows + which * half_rows, half_rows), half_rows
        )

    load_wa = pltpu.make_async_copy(wa, wfull.at[shard(t)], wsem.at[6])
    load_wo = pltpu.make_async_copy(wo, wobuf, wsem.at[7])
    load_wa.start()
    load_wo.start()

    def block_at(index):
        return pl.ds(pl.multiple_of(index * own, own), own)

    x = x_ref[...].astype(jnp.float32)
    held[block_at(t), :] = (rms_scale(x) * gain_ref[...]).astype(jnp.bfloat16)
    for row, ref in ((0, kg_ref), (1, qg_ref)):
        for h in range(heads):
            for m in range(2):
                at = (h * 2 + m) * comp
                gains[row : row + 1, at : at + comp] = ref[m : m + 1, :]

    barrier = pltpu.get_barrier_semaphore()

    def hello(where):
        pl.semaphore_signal(barrier, inc=1, device_id=where, device_id_type=MESH)

    for peer in (near, away, diag):
        hello({"tp": peer})
    for peer in (t, near, away, diag):
        hello({"sp": mate, "tp": peer})

    @pl.when(has_up)
    def _():
        hello({"sp": s + 2})

    @pl.when(has_down)
    def _():
        hello({"sp": s - 2})

    @pl.when((side == 1) & has_up)
    def _():
        hello({"sp": s + 1})

    @pl.when((side == 0) & has_down)
    def _():
        hello({"sp": s - 1})

    pl.semaphore_wait(barrier, 7 + ups + downs + side * ups + (1 - side) * downs)

    part = own // CHUNKS

    def chunk_at(index, c):
        return pl.ds(pl.multiple_of(index * own + c * part, part), part)

    def far_copy(c):
        spot = held.at[chunk_at(t, c)]
        return remote(spot, spot, far_send.at[c], far_recv.at[c], {"tp": away})

    def forward(c):
        spot = held.at[chunk_at(away, c)]
        return remote(spot, spot, fwd_send.at[c], fwd_recv.at[c], {"tp": near})

    far_copies = [far_copy(c) for c in range(CHUNKS)]
    forwards = [forward(c) for c in range(CHUNKS)]
    mine = held.at[block_at(t)]
    near_copy = remote(mine, mine, near_sem.at[0], near_sem.at[1], {"tp": near})
    near_copy.start()
    for copy in far_copies:
        copy.start()

    w_near = remote(wa, wfull.at[shard(t)], w_send.at[0], w_recv.at[0], {"tp": near})
    w_far = remote(
        wa.at[pl.ds(pl.multiple_of(side * half_rows, half_rows), half_rows)],
        wfull.at[part_of(t, side)], w_send.at[1], w_recv.at[1], {"tp": away},
    )

    def w_pass(which, slot):
        spot = wfull.at[part_of(away, which)]
        return remote(spot, spot, w_send.at[slot], w_recv.at[slot], {"tp": near})

    w_side_spot = wfull.at[part_of(away, side)]
    w_side = remote(w_side_spot, w_side_spot, w_send.at[2], w_recv.at[2], mate_id)

    def slot_of(lev, pair):
        return lev * 2 + pair

    def group_of(lev, pair, which):
        return (lev * 2 + pair) * 2 + which

    def side_rows(which):
        return pl.ds(pl.multiple_of(which * half, half), half)

    def up_copy(lev, pair, which):
        spot = kvb.at[slot_of(lev, pair), side_rows(which)]
        g = group_of(lev, pair, which)
        return remote(spot, spot, up_send.at[g], kv_recv.at[g], up_id)

    def give_copy(pair):
        return remote(
            give_kv.at[pair], kvb.at[slot_of(level, pair), side_rows(side)],
            gk_send.at[pair], kv_recv.at[group_of(level, pair, side)], mate_id,
        )

    def q_rows(which, pair):
        return pl.ds(pl.multiple_of(which * rows + pair * half, half), half)

    def giveq_copy(pair):
        return remote(
            give_q.at[pair], qb.at[q_rows(side, pair)], gq_send.at[pair], q_recv.at[pair], mate_id
        )

    def split(values):
        low, high = values[:, :head_cols], values[:, head_cols:]
        return jnp.where(side == 0, low, high), jnp.where(side == 0, high, low)

    def pair_rows(pair):
        return pl.ds(pl.multiple_of(pair * half, half), half)

    def scaled(block, i, gain_row, factor):
        res = jnp.dot(block, wbuf[i], preferred_element_type=jnp.float32).astype(jnp.bfloat16)
        wide = res.astype(jnp.float32)
        return (wide * group_scale(wide, comp) * (gains[gain_row : gain_row + 1] * factor)).astype(
            jnp.bfloat16
        )

    def project_kv(pair):
        block = held[pair_rows(pair)]
        slot = slot_of(level, pair)
        for i in range(2):
            if i == 0:
                res = scaled(block, 0, 0, 1.0)
            else:
                res = jnp.dot(block, wbuf[1], preferred_element_type=jnp.float32).astype(
                    jnp.bfloat16
                )
            keep, give = split(res)
            cols = slice(i * head_cols, (i + 1) * head_cols)
            kvb[slot, side_rows(side), cols] = keep
            give_kv[pair, :, cols] = give

        give_copy(pair).start()

        @pl.when(has_up)
        def _():
            up_copy(level, pair, side).start()

    def project_q(pair):
        block = held[pair_rows(pair)]
        keep, give = split(scaled(block, 2, 1, comp ** (-0.5)))
        qb[q_rows(side, pair)] = keep
        give_q[pair] = give
        giveq_copy(pair).start()

    def project_conv(pair):
        block = held[pair_rows(pair)]
        for i in range(3):
            cbuf[pair_rows(pair), i * channels : (i + 1) * channels] = jnp.dot(
                block, wbuf[3 + i], preferred_element_type=jnp.float32
            ).astype(jnp.bfloat16)

    def await_group(lev, pair, which):
        up_copy(lev, pair, which).wait_recv()

        @pl.when(has_up)
        def _():
            up_copy(lev, pair, which).start()

    def await_pair(lev, pair):
        await_group(lev, pair, side)
        await_group(lev, pair, 1 - side)

    loads[0].wait()
    loads[1].wait()
    near_copy.wait_recv()
    project_kv(first)
    w_near.start()
    w_far.start()
    loads[2].wait()
    project_q(first)
    for load in loads[3:]:
        load.wait()
    project_conv(first)
    await_group(level, first, 1 - side)

    @pl.when(has_down)
    def _():
        await_pair(level - 1, first)

    for c in range(CHUNKS):
        far_copies[c].wait_recv()
        forwards[c].start()
    for copy in forwards:
        copy.wait_recv()
    project_kv(second)
    project_q(second)
    project_conv(second)

    tail_copy = remote(
        cbuf.at[pl.ds(rows - EDGE, EDGE), pl.ds(0, 2 * channels)], tail,
        tail_sem.at[0], tail_sem.at[1], {"sp": jnp.minimum(s + 1, sp - 1)},
    )

    @pl.when(s < sp - 1)
    def _():
        tail_copy.start()

    await_group(level, second, 1 - side)
    giveq_copy(0).wait_recv()
    giveq_copy(1).wait_recv()

    queries = 2 * rows
    lane = lax.broadcasted_iota(jnp.int32, (queries, both), 1)
    for h in range(per):
        q = qb[:, h * both : (h + 1) * both]
        zero = jnp.zeros_like(q)
        qpad[h, :queries] = jnp.where(lane < comp, q, zero)
        qpad[h, queries:] = jnp.where(lane < comp, zero, q)
    top[...] = jnp.full_like(top, -1e30)
    total[...] = jnp.zeros_like(total)
    acc[...] = jnp.zeros_like(acc)
    tile = min(TILE, half)

    def update(h, k, v, at, mask):
        scores = lax.dot_general(
            k, qpad[h, at], (((1,), (1,)), ((), ())), preferred_element_type=jnp.float32
        )
        if mask is not None:
            kpos = lax.broadcasted_iota(jnp.int32, scores.shape, 0)
            qpos = mask + lax.broadcasted_iota(jnp.int32, scores.shape, 1)
            scores = jnp.where(kpos <= qpos, scores, -1e30)
        old = top[h : h + 1, at]
        new = jnp.maximum(old, jnp.max(scores, axis=0, keepdims=True))
        p = jnp.exp(scores - new)
        factor = jnp.exp(old - new)
        top[h : h + 1, at] = new
        total[h : h + 1, at] = total[h : h + 1, at] * factor + jnp.sum(p, axis=0, keepdims=True)
        acc[h, :, at] = acc[h, :, at] * factor + lax.dot_general(
            v, p.astype(jnp.bfloat16), (((0,), (0,)), ((), ())),
            preferred_element_type=jnp.float32,
        )

    def key_value(piece, h):
        k = piece[:, h * both : (h + 1) * both]
        v = piece[:, head_cols + h * vsize : head_cols + (h + 1) * vsize]
        return k, v

    def absorb(lev, pair):
        slot = slot_of(lev, pair)
        for h in range(per):
            for which in range(2):
                piece = kvb[slot, which * half : (which + 1) * half]
                k, v = key_value(piece, h)
                for start in range(0, 2 * queries, tile):
                    update(h, k, v, slice(start, start + tile), None)

    def absorb_diag():
        for h in range(per):
            for block in range(4):
                which, pair = block // 2, block % 2
                piece = kvb[slot_of(level, pair), which * half : (which + 1) * half]
                k, v = key_value(piece, h)
                base = block * half
                for m in range(2):
                    for start in range(base, queries, tile):
                        at = slice(m * queries + start, m * queries + start + tile)
                        update(h, k, v, at, start - base if start < base + half else None)

    @pl.loop(2, level + 1)
    def _(j):
        await_pair(level - j, first)
        absorb(level - j + 1, first)

    def product(ref):
        gate = ref[:, :channels].astype(jnp.float32)
        other = ref[:, channels : 2 * channels].astype(jnp.float32)
        return (gate * other).astype(jnp.bfloat16).astype(jnp.float32)

    padded[EDGE:] = product(cbuf)

    @pl.when(s > 0)
    def _():
        tail_copy.wait_recv()
        padded[:EDGE] = product(tail)

    @pl.when(s == 0)
    def _():
        padded[:EDGE] = jnp.zeros((EDGE, channels), jnp.float32)

    count = taps_ref.shape[0]
    conv = jnp.zeros((rows, channels), jnp.float32)
    for tap in range(count):
        begin = EDGE - count + 1 + tap
        conv = conv + taps_ref[tap : tap + 1] * padded[begin : begin + rows]
    gated = cbuf[:, 2 * channels :].astype(jnp.float32) * conv
    cvout[...] = (gated * group_scale(gated, GROUP) * cgain_ref[...]).astype(jnp.bfloat16)
    load_wo.wait()

    def partial(target):
        return jnp.dot(cvout[block_at(target), :], wobuf[...], preferred_element_type=jnp.float32)

    cross_copy = remote(cross, cross_in, cross_send, cross_recv, {"tp": near})
    fin_copy = remote(fin, fin_in, fin_send, fin_recv, {"tp": near})
    far_sum = remote(far, far_in, fs_send, fs_recv, {"tp": away})
    cross[...] = partial(diag).astype(jnp.bfloat16)
    cross_copy.start()
    fin[...] = partial(near).astype(jnp.bfloat16)
    fin_copy.start()
    out_ref[...] = partial(t)
    toward = partial(away)
    cross_copy.wait_recv()
    far[...] = (toward + cross_in[...].astype(jnp.float32)).astype(jnp.bfloat16)
    far_sum.start()

    @pl.when(has_down)
    def _():
        absorb(0, first)

    absorb_diag()

    @pl.when(has_down)
    def _():
        await_pair(level - 1, second)
        absorb(level - 1, second)

    w_far.wait_recv()
    w_side.start()
    w_pass(side, 3).start()

    @pl.loop(2, level + 1)
    def _(j):
        await_pair(level - j, second)
        absorb(level - j, second)

    w_side.wait_recv()
    w_pass(1 - side, 4).start()

    for h in range(per):
        inverse = 1.0 / total[h : h + 1]
        mapped = acc[h] * inverse
        attn = mapped[:, :queries] - lam_ref[side * per + h] * mapped[:, queries:]
        scale = lax.rsqrt(jnp.mean(attn * attn, axis=0, keepdims=True) + eps)
        result = (attn * scale).T * sub_ref[...]
        obuf[:, h * vsize : (h + 1) * vsize] = result.astype(jnp.bfloat16)
        logs = top[h : h + 1] + jnp.log(total[h : h + 1])
        for m in range(2):
            low = logs[:, m * queries : m * queries + rows]
            high = logs[:, m * queries + rows : (m + 1) * queries]
            log_ref[side * per + h, m : m + 1, :] = jnp.where(side == 0, low, high)
            lout[h, m : m + 1, :] = jnp.where(side == 0, high, low)

    me8 = t * 2 + side

    def piece_rows(which, target):
        return pl.ds(pl.multiple_of(which * rows + target * own, own), own)

    def o_copy(which, target, index):
        return remote(
            obuf.at[piece_rows(which, target)], hin.at[me8], o_send.at[index], o_recv.at[me8],
            {"sp": level * 2 + which, "tp": target},
        )

    def o_wait(which, source, index):
        spot = hin.at[source * 2 + which]
        return remote(spot, spot, o_send.at[index], o_recv.at[source * 2 + which], mate_id)

    peers = [(1 - side, diag), (1 - side, away), (side, diag), (side, away)]
    peers += [(1 - side, t), (1 - side, near), (side, near)]
    for index, (which, target) in enumerate(peers):
        o_copy(which, target, index).start()
    log_copy = remote(lout, lin, log_sem.at[0], log_sem.at[1], mate_id)
    log_copy.start()
    hin[me8] = obuf[piece_rows(side, t)]
    fin_copy.wait_recv()
    far_sum.wait_recv()
    out_ref[...] += fin_in[...].astype(jnp.float32) + far_in[...].astype(jnp.float32)
    load_wa.wait()
    w_near.wait_recv()
    w_pass(side, 3).wait_recv()
    w_pass(1 - side, 4).wait_recv()
    for index, (which, source) in enumerate(peers):
        o_wait(which, source, index).wait_recv()
    lhs = jnp.concatenate([hin[i] for i in range(2 * tp)], axis=1)
    out_ref[...] += jnp.dot(lhs, wfull[...], preferred_element_type=jnp.float32)
    log_copy.wait_recv()
    for h in range(per):
        log_ref[(1 - side) * per + h] = lin[h]

    near_copy.wait_send()
    for copy in far_copies + forwards:
        copy.wait_send()
    for pair in range(2):
        give_copy(pair).wait_send()
        giveq_copy(pair).wait_send()
    for copy in (w_near, w_far, w_side, w_pass(side, 3), w_pass(1 - side, 4)):
        copy.wait_send()
    for copy in (cross_copy, fin_copy, far_sum, log_copy):
        copy.wait_send()
    for index, (which, target) in enumerate(peers):
        o_copy(which, target, index).wait_send()

    @pl.when(has_up)
    def _():
        @pl.loop(0, level + 1)
        def _(lev):
            for pair in range(2):
                for which in range(2):
                    up_copy(lev, pair, which).wait_send()

    @pl.when(s < sp - 1)
    def _():
        tail_copy.wait_send()


def vmem():
    return pl.BlockSpec(memory_space=pltpu.VMEM)


def on_device(
    inputs, norm_gain, w_query, w_key, w_value, query_gain, key_gain, lambdas, sub_gain,
    w_gate_b, w_gate_c, w_conv_in, conv_taps, conv_gain, w_out_att, w_out_conv,
):
    heads = lambdas.shape[0]
    comp = query_gain.shape[1]
    vsize = sub_gain.shape[0]
    channels = conv_gain.shape[0]
    own, width = inputs.shape
    tp = lax.axis_size("tp")
    sp = lax.axis_size("sp")
    rows = own * tp
    half = rows // 2
    qcols = heads * 2 * comp
    mine = qcols // 2
    per = heads // 2
    dma = pltpu.SemaphoreType.DMA
    bf, f32 = jnp.bfloat16, jnp.float32
    weights = (w_key, w_value, w_query, w_gate_c, w_conv_in, w_gate_b, w_out_att, w_out_conv)
    groups = sp // 2 * 4
    piece = pltpu.VMEM((own, width), bf)
    any_spec = pl.BlockSpec(memory_space=pl.ANY)
    mixed, log_sums = pl.pallas_call(
        functools.partial(layer, sp, tp, comp, heads),
        out_shape=(
            jax.ShapeDtypeStruct((own, width), f32),
            jax.ShapeDtypeStruct((heads, 2, rows), f32),
        ),
        in_specs=[vmem()] * 4 + [pl.BlockSpec(memory_space=pltpu.SMEM)] + [vmem()] * 3
        + [any_spec] * 8,
        out_specs=(vmem(), vmem()),
        scratch_shapes=[
            pltpu.VMEM((rows, width), bf),
            pltpu.VMEM((6, width, qcols), bf),
            pltpu.VMEM((tp * w_out_att.shape[0], width), bf),
            pltpu.VMEM(w_out_conv.shape, bf),
            pltpu.VMEM((8, qcols), f32),
            pltpu.VMEM((sp, 2 * half, 2 * mine), bf),
            pltpu.VMEM((2 * rows, mine), bf),
            pltpu.VMEM((2, half, 2 * mine), bf),
            pltpu.VMEM((2, half, mine), bf),
            pltpu.VMEM((per, 4 * rows, 2 * comp), bf),
            pltpu.VMEM((per, 4 * rows), f32),
            pltpu.VMEM((per, 4 * rows), f32),
            pltpu.VMEM((per, vsize, 4 * rows), f32),
            pltpu.VMEM((rows, 3 * channels), bf),
            pltpu.VMEM((EDGE, 2 * channels), bf),
            pltpu.VMEM((EDGE + rows, channels), f32),
            pltpu.VMEM((rows, channels), bf),
            piece, piece, piece, piece, piece, piece,
            pltpu.VMEM((2 * rows, per * vsize), bf),
            pltpu.VMEM((2 * tp, own, per * vsize), bf),
            pltpu.VMEM((per, 2, rows), f32),
            pltpu.VMEM((per, 2, rows), f32),
            dma((8,)), dma((2,)), dma((CHUNKS,)), dma((CHUNKS,)), dma((CHUNKS,)), dma((CHUNKS,)),
            dma((groups,)), dma((groups,)), dma((2,)), dma((2,)), dma((2,)), dma((2,)),
            dma((5,)), dma((5,)), dma(()), dma(()), dma(()), dma(()), dma(()), dma(()),
            dma((7,)), dma((2 * tp,)), dma((2,)),
        ],
        compiler_params=pltpu.CompilerParams(
            collective_id=0, has_side_effects=True, vmem_limit_bytes=VMEM_LIMIT
        ),
        name="layer",
    )(
        inputs, norm_gain[None], query_gain, key_gain, lambdas, sub_gain[None], conv_taps,
        conv_gain[None], *weights,
    )
    return (mixed, log_sums)


def solution(mesh):
    in_specs = (
        P(("sp", "tp"), None),
        P(),
        P(None, "tp"),
        P(None, "tp"),
        P(None, "tp"),
        P(),
        P(),
        P("tp"),
        P(),
        P(None, "tp"),
        P(None, "tp"),
        P(None, "tp"),
        P(None, "tp"),
        P("tp"),
        P("tp", None),
        P("tp", None),
    )
    out_specs = (P(("sp", "tp"), None), P("tp", None, "sp"))
    return jax.shard_map(
        on_device, mesh=mesh, in_specs=in_specs, out_specs=out_specs, check_vma=False
    )
```

```python
import functools

import jax
import jax.numpy as jnp
from jax import lax
from jax.experimental import pallas as pl
from jax.experimental.pallas import tpu as pltpu
from jax.sharding import PartitionSpec as P

GROUP = 64
eps = 1e-06
MESH = pl.DeviceIdType.MESH
VMEM_LIMIT = 62 * 1024 * 1024
CHUNKS = 4
EDGE = 16
TILE = 128


def rms_scale(values):
    return values * lax.rsqrt(jnp.mean(values * values, axis=-1, keepdims=True) + eps)


def flip(index, bit):
    return index + bit - 2 * bit * lax.rem(index // bit, 2)


def remote(src, dst, send, recv, where):
    return pltpu.make_async_remote_copy(
        src_ref=src, dst_ref=dst, send_sem=send, recv_sem=recv, device_id=where,
        device_id_type=MESH,
    )


def group_scale(values, size):
    lanes = values.shape[1]
    row = lax.broadcasted_iota(jnp.int32, (lanes, lanes), 0) // size
    col = lax.broadcasted_iota(jnp.int32, (lanes, lanes), 1) // size
    ones = jnp.where(row == col, 1.0, 0.0).astype(jnp.bfloat16)
    squares = values * values
    high = squares.astype(jnp.bfloat16)
    low = (squares - high.astype(jnp.float32)).astype(jnp.bfloat16)
    sums = jnp.dot(high, ones, preferred_element_type=jnp.float32) + jnp.dot(
        low, ones, preferred_element_type=jnp.float32
    )
    return lax.rsqrt(sums * (1.0 / size) + eps)


def layer(
    sp, tp, comp, heads,
    x_ref, gain_ref, qg_ref, kg_ref, lam_ref, sub_ref, taps_ref, cgain_ref,
    wk, wv, wq, wc, wi, wb, wa, wo,
    out_ref, log_ref,
    held, wbuf, wfull, wobuf, gains, kvb, vt, qb, give_kv, give_q, qpad, top, total, acc, cbuf, tail,
    padded, cvout, cross, fin, far, cross_in, fin_in, far_in, obuf, hin, lout, lin,
    wsem, near_sem, far_send, far_recv, fwd_send, fwd_recv, up_send, kv_recv, gk_send, gq_send,
    q_recv, tail_sem, w_send, w_recv, cross_send, cross_recv, fin_send, fin_recv, fs_send, fs_recv,
    o_send, o_recv, log_sem,
):
    s = lax.axis_index("sp")
    t = lax.axis_index("tp")
    level, side = s // 2, lax.rem(s, 2)
    levels = sp // 2
    mate = level * 2 + 1 - side
    near, away = flip(t, 1), flip(t, 2)
    diag = flip(near, 2)
    first, second = t // 2, 1 - t // 2
    own = x_ref.shape[0]
    rows = own * tp
    half = rows // 2
    head_cols = heads * 2 * comp // 2
    per = heads // 2
    vsize = sub_ref.shape[1]
    both = 2 * comp
    channels = cgain_ref.shape[1]
    has_up, has_down = level < levels - 1, level > 0
    ups, downs = has_up.astype(jnp.int32), has_down.astype(jnp.int32)
    up_id = {"sp": jnp.minimum(s + 2, sp - 2 + side)}
    mate_id = {"sp": mate}

    loads = [
        pltpu.make_async_copy(w, wbuf.at[i], wsem.at[i])
        for i, w in enumerate((wk, wv, wq, wc, wi, wb))
    ]
    for load in loads:
        load.start()
    wa_rows = wa.shape[0]
    half_rows = wa_rows // 2

    def shard(index):
        return pl.ds(pl.multiple_of(index * wa_rows, wa_rows), wa_rows)

    def part_of(index, which):
        return pl.ds(
            pl.multiple_of(index * wa_rows + which * half_rows, half_rows), half_rows
        )

    load_wa = pltpu.make_async_copy(wa, wfull.at[shard(t)], wsem.at[6])
    load_wo = pltpu.make_async_copy(wo, wobuf, wsem.at[7])
    load_wa.start()
    load_wo.start()

    def block_at(index):
        return pl.ds(pl.multiple_of(index * own, own), own)

    phase("norm")
    x = x_ref[...].astype(jnp.float32)
    held[block_at(t), :] = (rms_scale(x) * gain_ref[...]).astype(jnp.bfloat16)
    for row, ref in ((0, kg_ref), (1, qg_ref)):
        for h in range(heads):
            for m in range(2):
                at = (h * 2 + m) * comp
                gains[row : row + 1, at : at + comp] = ref[m : m + 1, :]

    phase("barrier")
    barrier = pltpu.get_barrier_semaphore()

    def hello(where):
        pl.semaphore_signal(barrier, inc=1, device_id=where, device_id_type=MESH)

    for peer in (near, away, diag):
        hello({"tp": peer})
    for peer in (t, near, away, diag):
        hello({"sp": mate, "tp": peer})

    @pl.when(has_up)
    def _():
        hello({"sp": s + 2})

    @pl.when(has_down)
    def _():
        hello({"sp": s - 2})

    @pl.when((side == 1) & has_up)
    def _():
        hello({"sp": s + 1})

    @pl.when((side == 0) & has_down)
    def _():
        hello({"sp": s - 1})

    pl.semaphore_wait(barrier, 7 + ups + downs + side * ups + (1 - side) * downs)

    phase("defs")
    part = own // CHUNKS

    def chunk_at(index, c):
        return pl.ds(pl.multiple_of(index * own + c * part, part), part)

    def far_copy(c):
        spot = held.at[chunk_at(t, c)]
        return remote(spot, spot, far_send.at[c], far_recv.at[c], {"tp": away})

    def forward(c):
        spot = held.at[chunk_at(away, c)]
        return remote(spot, spot, fwd_send.at[c], fwd_recv.at[c], {"tp": near})

    far_copies = [far_copy(c) for c in range(CHUNKS)]
    forwards = [forward(c) for c in range(CHUNKS)]
    mine = held.at[block_at(t)]
    near_copy = remote(mine, mine, near_sem.at[0], near_sem.at[1], {"tp": near})
    near_copy.start()
    for copy in far_copies:
        copy.start()

    w_near = remote(wa, wfull.at[shard(t)], w_send.at[0], w_recv.at[0], {"tp": near})
    w_far = remote(
        wa.at[pl.ds(pl.multiple_of(side * half_rows, half_rows), half_rows)],
        wfull.at[part_of(t, side)], w_send.at[1], w_recv.at[1], {"tp": away},
    )

    def w_pass(which, slot):
        spot = wfull.at[part_of(away, which)]
        return remote(spot, spot, w_send.at[slot], w_recv.at[slot], {"tp": near})

    w_side_spot = wfull.at[part_of(away, side)]
    w_side = remote(w_side_spot, w_side_spot, w_send.at[2], w_recv.at[2], mate_id)

    def slot_of(lev, pair):
        return lev * 2 + pair

    def group_of(lev, pair, which):
        return (lev * 2 + pair) * 2 + which

    def side_rows(which):
        return pl.ds(pl.multiple_of(which * half, half), half)

    def up_copy(lev, pair, which):
        spot = kvb.at[slot_of(lev, pair), side_rows(which)]
        g = group_of(lev, pair, which)
        return remote(spot, spot, up_send.at[g], kv_recv.at[g], up_id)

    def give_copy(pair):
        return remote(
            give_kv.at[pair], kvb.at[slot_of(level, pair), side_rows(side)],
            gk_send.at[pair], kv_recv.at[group_of(level, pair, side)], mate_id,
        )

    def q_rows(which, pair):
        return pl.ds(pl.multiple_of(which * rows + pair * half, half), half)

    def giveq_copy(pair):
        return remote(
            give_q.at[pair], qb.at[q_rows(side, pair)], gq_send.at[pair], q_recv.at[pair], mate_id
        )

    def split(values):
        low, high = values[:, :head_cols], values[:, head_cols:]
        return jnp.where(side == 0, low, high), jnp.where(side == 0, high, low)

    def pair_rows(pair):
        return pl.ds(pl.multiple_of(pair * half, half), half)

    def scaled(block, i, gain_row, factor):
        res = jnp.dot(block, wbuf[i], preferred_element_type=jnp.float32).astype(jnp.bfloat16)
        wide = res.astype(jnp.float32)
        return (wide * group_scale(wide, comp) * (gains[gain_row : gain_row + 1] * factor)).astype(
            jnp.bfloat16
        )

    def project_kv(pair):
        block = held[pair_rows(pair)]
        slot = slot_of(level, pair)
        for i in range(2):
            if i == 0:
                res = scaled(block, 0, 0, 1.0)
            else:
                res = jnp.dot(block, wbuf[1], preferred_element_type=jnp.float32).astype(
                    jnp.bfloat16
                )
            keep, give = split(res)
            cols = slice(i * head_cols, (i + 1) * head_cols)
            kvb[slot, side_rows(side), cols] = keep
            give_kv[pair, :, cols] = give

        give_copy(pair).start()

        @pl.when(has_up)
        def _():
            up_copy(level, pair, side).start()

    def project_q(pair):
        block = held[pair_rows(pair)]
        keep, give = split(scaled(block, 2, 1, comp ** (-0.5)))
        qb[q_rows(side, pair)] = keep
        give_q[pair] = give
        giveq_copy(pair).start()

    def project_conv(pair):
        block = held[pair_rows(pair)]
        for i in range(3):
            cbuf[pair_rows(pair), i * channels : (i + 1) * channels] = jnp.dot(
                block, wbuf[3 + i], preferred_element_type=jnp.float32
            ).astype(jnp.bfloat16)

    def await_group(lev, pair, which):
        up_copy(lev, pair, which).wait_recv()

        @pl.when(has_up)
        def _():
            up_copy(lev, pair, which).start()

    def await_pair(lev, pair):
        await_group(lev, pair, side)
        await_group(lev, pair, 1 - side)

    phase("wait_kv_weights")
    loads[0].wait()
    loads[1].wait()
    phase("wait_near")
    near_copy.wait_recv()
    phase("kv_first")
    project_kv(first)
    w_near.start()
    phase("q_first")
    loads[2].wait()
    project_q(first)
    phase("conv_first")
    for load in loads[3:]:
        load.wait()
    project_conv(first)
    phase("mate_first")
    await_group(level, first, 1 - side)

    phase("below_first")
    @pl.when(has_down)
    def _():
        await_pair(level - 1, first)

    phase("far_wait")
    for c in range(CHUNKS):
        far_copies[c].wait_recv()
        forwards[c].start()
    w_far.start()
    for copy in forwards:
        copy.wait_recv()
    phase("kv_second")
    project_kv(second)
    phase("q_second")
    project_q(second)
    phase("below_first2")

    @pl.when(level > 1)
    def _():
        await_pair(level - 2, first)

    phase("conv_second")
    project_conv(second)

    tail_copy = remote(
        cbuf.at[pl.ds(rows - EDGE, EDGE), pl.ds(0, 2 * channels)], tail,
        tail_sem.at[0], tail_sem.at[1], {"sp": jnp.minimum(s + 1, sp - 1)},
    )

    @pl.when(s < sp - 1)
    def _():
        tail_copy.start()

    phase("mate_second")
    await_group(level, second, 1 - side)
    giveq_copy(0).wait_recv()
    giveq_copy(1).wait_recv()

    phase("qpad")
    queries = 2 * rows
    lane = lax.broadcasted_iota(jnp.int32, (queries, both), 1)
    for h in range(per):
        q = qb[:, h * both : (h + 1) * both]
        zero = jnp.zeros_like(q)
        qpad[h, :queries] = jnp.where(lane < comp, q, zero)
        qpad[h, queries:] = jnp.where(lane < comp, zero, q)
    top[...] = jnp.full_like(top, -1e30)
    total[...] = jnp.zeros_like(total)
    acc[...] = jnp.zeros_like(acc)
    tile = min(TILE, half)

    def run_tiles(work):
        def score(item):
            h, keys, values, at, mask = item
            return lax.dot_general(
                keys(), qpad[h, at], (((1,), (1,)), ((), ())), preferred_element_type=jnp.float32
            )

        ahead = score(work[0])
        for index, (h, keys, values, at, mask) in enumerate(work):
            scores = ahead
            if index + 1 < len(work):
                ahead = score(work[index + 1])
            if mask is not None:
                kpos = lax.broadcasted_iota(jnp.int32, scores.shape, 0)
                qpos = mask + lax.broadcasted_iota(jnp.int32, scores.shape, 1)
                scores = jnp.where(kpos <= qpos, scores, -1e30)
            old = top[h : h + 1, at]
            new = jnp.maximum(old, jnp.max(scores, axis=0, keepdims=True))
            p = jnp.exp(scores - new)
            factor = jnp.exp(old - new)
            top[h : h + 1, at] = new
            total[h : h + 1, at] = total[h : h + 1, at] * factor + jnp.sum(
                p, axis=0, keepdims=True
            )
            acc[h, :, at] = acc[h, :, at] * factor + jnp.dot(
                values(), p.astype(jnp.bfloat16), preferred_element_type=jnp.float32
            )

    def key_part(slot, h, begin, size):
        return lambda: kvb[slot, begin : begin + size, h * both : (h + 1) * both]

    def value_part(which, h, begin, size):
        return lambda: vt[which, h, :, begin : begin + size]

    def turn_values(slot, which):
        for h in range(per):
            cols = slice(head_cols + h * vsize, head_cols + (h + 1) * vsize)
            vt[which, h] = kvb[slot, :, cols].T

    def absorb(lev, pair):
        slot = slot_of(lev, pair)
        turn_values(slot, 0)
        run_tiles(
            [
                (
                    h, key_part(slot, h, which * half, half),
                    value_part(0, h, which * half, half), slice(start, start + tile), None,
                )
                for h in range(per)
                for start in range(0, 2 * queries, tile)
                for which in range(2)
            ]
        )

    def absorb_diag():
        work = []
        for pair in range(2):
            turn_values(slot_of(level, pair), pair)
        for h in range(per):
            for block in range(4):
                which, pair = block // 2, block % 2
                base = block * half
                for m in range(2):
                    for start in range(base, queries, tile):
                        at = slice(m * queries + start, m * queries + start + tile)
                        inside = start < base + half
                        size = min(start - base + tile, half) if inside else half
                        work.append(
                            (
                                h, key_part(slot_of(level, pair), h, which * half, size),
                                value_part(pair, h, which * half, size), at,
                                start - base if inside else None,
                            )
                        )
        run_tiles(work)

    phase("absorb1")

    @pl.when(has_down)
    def _():
        absorb(level - 1, first)

    phase("conv")
    def product(ref):
        gate = ref[:, :channels].astype(jnp.float32)
        other = ref[:, channels : 2 * channels].astype(jnp.float32)
        return (gate * other).astype(jnp.bfloat16).astype(jnp.float32)

    padded[EDGE:] = product(cbuf)

    @pl.when(s > 0)
    def _():
        tail_copy.wait_recv()
        padded[:EDGE] = product(tail)

    @pl.when(s == 0)
    def _():
        padded[:EDGE] = jnp.zeros((EDGE, channels), jnp.float32)

    count = taps_ref.shape[0]
    conv = jnp.zeros((rows, channels), jnp.float32)
    for tap in range(count):
        begin = EDGE - count + 1 + tap
        conv = conv + taps_ref[tap : tap + 1] * padded[begin : begin + rows]
    gated = cbuf[:, 2 * channels :].astype(jnp.float32) * conv
    cvout[...] = (gated * group_scale(gated, GROUP) * cgain_ref[...]).astype(jnp.bfloat16)
    load_wo.wait()

    def partial(target):
        return jnp.dot(cvout[block_at(target), :], wobuf[...], preferred_element_type=jnp.float32)

    cross_copy = remote(cross, cross_in, cross_send, cross_recv, {"tp": near})
    fin_copy = remote(fin, fin_in, fin_send, fin_recv, {"tp": near})
    far_sum = remote(far, far_in, fs_send, fs_recv, {"tp": away})
    phase("partial")
    cross[...] = partial(diag).astype(jnp.bfloat16)
    cross_copy.start()
    fin[...] = partial(near).astype(jnp.bfloat16)
    fin_copy.start()
    out_ref[...] = partial(t)
    toward = partial(away)
    cross_copy.wait_recv()
    far[...] = (toward + cross_in[...].astype(jnp.float32)).astype(jnp.bfloat16)
    far_sum.start()

    phase("w_far")
    w_far.wait_recv()
    w_side.start()
    w_pass(side, 3).start()
    phase("near_loop")

    @pl.loop(3, level + 1)
    def _(j):
        await_pair(level - j, first)
        absorb(level - j + 1, first)

    @pl.when(level > 1)
    def _():
        absorb(0, first)

    phase("below_second")

    @pl.when(has_down)
    def _():
        await_pair(level - 1, second)

    phase("diag")
    absorb_diag()

    @pl.when(has_down)
    def _():
        absorb(level - 1, second)

    phase("far_loop")
    @pl.loop(2, level + 1)
    def _(j):
        await_pair(level - j, second)
        absorb(level - j, second)

    phase("w_side")
    w_side.wait_recv()
    w_pass(1 - side, 4).start()

    phase("finalize")
    for h in range(per):
        inverse = 1.0 / total[h : h + 1]
        mapped = acc[h] * inverse
        attn = mapped[:, :queries] - lam_ref[side * per + h] * mapped[:, queries:]
        scale = lax.rsqrt(jnp.mean(attn * attn, axis=0, keepdims=True) + eps)
        result = (attn * scale).T * sub_ref[...]
        obuf[:, h * vsize : (h + 1) * vsize] = result.astype(jnp.bfloat16)
        logs = top[h : h + 1] + jnp.log(total[h : h + 1])
        for m in range(2):
            low = logs[:, m * queries : m * queries + rows]
            high = logs[:, m * queries + rows : (m + 1) * queries]
            log_ref[side * per + h, m : m + 1, :] = jnp.where(side == 0, low, high)
            lout[h, m : m + 1, :] = jnp.where(side == 0, high, low)

    phase("send_o")
    me8 = t * 2 + side

    def piece_rows(which, target):
        return pl.ds(pl.multiple_of(which * rows + target * own, own), own)

    def o_copy(which, target, index):
        return remote(
            obuf.at[piece_rows(which, target)], hin.at[me8], o_send.at[index], o_recv.at[me8],
            {"sp": level * 2 + which, "tp": target},
        )

    def o_wait(which, source, index):
        spot = hin.at[source * 2 + which]
        return remote(spot, spot, o_send.at[index], o_recv.at[source * 2 + which], mate_id)

    peers = [(1 - side, diag), (1 - side, away), (side, diag), (side, away)]
    peers += [(1 - side, t), (1 - side, near), (side, near)]
    for index, (which, target) in enumerate(peers):
        o_copy(which, target, index).start()
    log_copy = remote(lout, lin, log_sem.at[0], log_sem.at[1], mate_id)
    log_copy.start()
    hin[me8] = obuf[piece_rows(side, t)]
    phase("conv_sum")
    fin_copy.wait_recv()
    far_sum.wait_recv()
    out_ref[...] += fin_in[...].astype(jnp.float32) + far_in[...].astype(jnp.float32)
    phase("w_wait")
    load_wa.wait()
    w_near.wait_recv()
    w_pass(side, 3).wait_recv()
    w_pass(1 - side, 4).wait_recv()
    phase("o_wait")
    for index, (which, source) in enumerate(peers):
        o_wait(which, source, index).wait_recv()
    phase("last_dot")
    lhs = jnp.concatenate([hin[i] for i in range(2 * tp)], axis=1)
    out_ref[...] += jnp.dot(lhs, wfull[...], preferred_element_type=jnp.float32)
    phase("log")
    log_copy.wait_recv()
    for h in range(per):
        log_ref[(1 - side) * per + h] = lin[h]

    phase("sends")
    near_copy.wait_send()
    for copy in far_copies + forwards:
        copy.wait_send()
    for pair in range(2):
        give_copy(pair).wait_send()
        giveq_copy(pair).wait_send()
    for copy in (w_near, w_far, w_side, w_pass(side, 3), w_pass(1 - side, 4)):
        copy.wait_send()
    for copy in (cross_copy, fin_copy, far_sum, log_copy):
        copy.wait_send()
    for index, (which, target) in enumerate(peers):
        o_copy(which, target, index).wait_send()

    @pl.when(has_up)
    def _():
        @pl.loop(0, level + 1)
        def _(lev):
            for pair in range(2):
                for which in range(2):
                    up_copy(lev, pair, which).wait_send()

    @pl.when(s < sp - 1)
    def _():
        tail_copy.wait_send()

    phase(None)


def phase(name):
    pass


def vmem():
    return pl.BlockSpec(memory_space=pltpu.VMEM)


def on_device(
    inputs, norm_gain, w_query, w_key, w_value, query_gain, key_gain, lambdas, sub_gain,
    w_gate_b, w_gate_c, w_conv_in, conv_taps, conv_gain, w_out_att, w_out_conv,
):
    heads = lambdas.shape[0]
    comp = query_gain.shape[1]
    vsize = sub_gain.shape[0]
    channels = conv_gain.shape[0]
    own, width = inputs.shape
    tp = lax.axis_size("tp")
    sp = lax.axis_size("sp")
    rows = own * tp
    half = rows // 2
    qcols = heads * 2 * comp
    mine = qcols // 2
    per = heads // 2
    dma = pltpu.SemaphoreType.DMA
    bf, f32 = jnp.bfloat16, jnp.float32
    weights = (w_key, w_value, w_query, w_gate_c, w_conv_in, w_gate_b, w_out_att, w_out_conv)
    groups = sp // 2 * 4
    piece = pltpu.VMEM((own, width), bf)
    any_spec = pl.BlockSpec(memory_space=pl.ANY)
    mixed, log_sums = pl.pallas_call(
        functools.partial(layer, sp, tp, comp, heads),
        out_shape=(
            jax.ShapeDtypeStruct((own, width), f32),
            jax.ShapeDtypeStruct((heads, 2, rows), f32),
        ),
        in_specs=[vmem()] * 4 + [pl.BlockSpec(memory_space=pltpu.SMEM)] + [vmem()] * 3
        + [any_spec] * 8,
        out_specs=(vmem(), vmem()),
        scratch_shapes=[
            pltpu.VMEM((rows, width), bf),
            pltpu.VMEM((6, width, qcols), bf),
            pltpu.VMEM((tp * w_out_att.shape[0], width), bf),
            pltpu.VMEM(w_out_conv.shape, bf),
            pltpu.VMEM((8, qcols), f32),
            pltpu.VMEM((sp, 2 * half, 2 * mine), bf),
            pltpu.VMEM((2, per, vsize, 2 * half), bf),
            pltpu.VMEM((2 * rows, mine), bf),
            pltpu.VMEM((2, half, 2 * mine), bf),
            pltpu.VMEM((2, half, mine), bf),
            pltpu.VMEM((per, 4 * rows, 2 * comp), bf),
            pltpu.VMEM((per, 4 * rows), f32),
            pltpu.VMEM((per, 4 * rows), f32),
            pltpu.VMEM((per, vsize, 4 * rows), f32),
            pltpu.VMEM((rows, 3 * channels), bf),
            pltpu.VMEM((EDGE, 2 * channels), bf),
            pltpu.VMEM((EDGE + rows, channels), f32),
            pltpu.VMEM((rows, channels), bf),
            piece, piece, piece, piece, piece, piece,
            pltpu.VMEM((2 * rows, per * vsize), bf),
            pltpu.VMEM((2 * tp, own, per * vsize), bf),
            pltpu.VMEM((per, 2, rows), f32),
            pltpu.VMEM((per, 2, rows), f32),
            dma((8,)), dma((2,)), dma((CHUNKS,)), dma((CHUNKS,)), dma((CHUNKS,)), dma((CHUNKS,)),
            dma((groups,)), dma((groups,)), dma((2,)), dma((2,)), dma((2,)), dma((2,)),
            dma((5,)), dma((5,)), dma(()), dma(()), dma(()), dma(()), dma(()), dma(()),
            dma((7,)), dma((2 * tp,)), dma((2,)),
        ],
        compiler_params=pltpu.CompilerParams(
            collective_id=0, has_side_effects=True, vmem_limit_bytes=VMEM_LIMIT
        ),
        name="layer",
    )(
        inputs, norm_gain[None], query_gain, key_gain, lambdas, sub_gain[None], conv_taps,
        conv_gain[None], *weights,
    )
    return (mixed, log_sums)


def solution(mesh):
    in_specs = (
        P(("sp", "tp"), None),
        P(),
        P(None, "tp"),
        P(None, "tp"),
        P(None, "tp"),
        P(),
        P(),
        P("tp"),
        P(),
        P(None, "tp"),
        P(None, "tp"),
        P(None, "tp"),
        P(None, "tp"),
        P("tp"),
        P("tp", None),
        P("tp", None),
    )
    out_specs = (P(("sp", "tp"), None), P("tp", None, "sp"))
    return jax.shard_map(
        on_device, mesh=mesh, in_specs=in_specs, out_specs=out_specs, check_vma=False
    )
```

```python
import functools

import jax
import jax.numpy as jnp
from jax import lax
from jax.experimental import pallas as pl
from jax.experimental.pallas import tpu as pltpu
from jax.sharding import PartitionSpec as P

GROUP = 64
eps = 1e-06
MESH = pl.DeviceIdType.MESH
VMEM_LIMIT = 62 * 1024 * 1024
CHUNKS = 4
EDGE = 16
TILE = 128
DEPTH = 2
W_PARTS = 2


def rms_scale(values):
    return values * lax.rsqrt(jnp.mean(values * values, axis=-1, keepdims=True) + eps)


def flip(index, bit):
    return index + bit - 2 * bit * lax.rem(index // bit, 2)


def remote(src, dst, send, recv, where):
    return pltpu.make_async_remote_copy(
        src_ref=src, dst_ref=dst, send_sem=send, recv_sem=recv, device_id=where,
        device_id_type=MESH,
    )


def group_scale(values, size):
    lanes = values.shape[1]
    row = lax.broadcasted_iota(jnp.int32, (lanes, lanes), 0) // size
    col = lax.broadcasted_iota(jnp.int32, (lanes, lanes), 1) // size
    ones = jnp.where(row == col, 1.0, 0.0).astype(jnp.bfloat16)
    squares = values * values
    high = squares.astype(jnp.bfloat16)
    low = (squares - high.astype(jnp.float32)).astype(jnp.bfloat16)
    sums = jnp.dot(high, ones, preferred_element_type=jnp.float32) + jnp.dot(
        low, ones, preferred_element_type=jnp.float32
    )
    return lax.rsqrt(sums * (1.0 / size) + eps)


def layer(
    sp, tp, comp, heads,
    x_ref, gain_ref, qg_ref, kg_ref, lam_ref, sub_ref, taps_ref, cgain_ref,
    wk, wv, wq, wc, wi, wb, wa, wo,
    out_ref, log_ref,
    held, wbuf, wfull, wobuf, gains, kvb, vt, qb, give_kv, give_q, qpad, top, total, acc, cbuf, tail,
    padded, cvout, lamb, cross, fin, far, cross_in, fin_in, far_in, obuf, hin, lout, lin,
    wsem, near_sem, far_send, far_recv, fwd_send, fwd_recv, up_send, kv_recv, gk_send, gq_send,
    q_recv, tail_sem, w_send, w_recv, cross_send, cross_recv, fin_send, fin_recv, fs_send, fs_recv,
    o_send, o_recv, log_send, log_recv, lam_sem, qs_send, qs_recv,
):
    s = lax.axis_index("sp")
    t = lax.axis_index("tp")
    level, side = s // 2, lax.rem(s, 2)
    levels = sp // 2
    mate = level * 2 + 1 - side
    near, away = flip(t, 1), flip(t, 2)
    diag = flip(near, 2)
    first, second = t // 2, 1 - t // 2
    own = x_ref.shape[0]
    rows = own * tp
    half = rows // 2
    head_cols = heads * 2 * comp // 2
    per = heads // 2
    vsize = sub_ref.shape[1]
    both = 2 * comp
    channels = cgain_ref.shape[1]
    has_up, has_down = level < levels - 1, level > 0

    def as_int(flag):
        return flag.astype(jnp.int32)

    ups, downs = as_int(has_up), as_int(has_down)
    mate_id = {"sp": mate}
    odd = lax.rem(t, 2)
    is_top, is_low = as_int(level == levels - 1), as_int(level == levels - 2)
    high_pair = is_top + is_low
    swapped = is_low * odd + is_top * (1 - odd)
    swaps = swapped == 1
    aside = is_low * (1 - odd) + is_top
    job_level = level + is_low * odd - is_top * (1 - odd)
    job_tp = t + swapped * (near - t)
    cross_sp = s + 2 * is_low - 2 * is_top
    cross_id = {"sp": cross_sp, "tp": near}
    up_id = {
        "sp": s + (1 - is_top) * (2 - 2 * is_low * (1 - odd)) - 2 * is_top * (1 - odd),
        "tp": t + aside * (near - t),
    }
    sends_own = is_top * odd == 0
    relays = is_top * (1 - odd) == 0
    groups = sp // 2 * 4

    loads = [
        pltpu.make_async_copy(w, wbuf.at[i], wsem.at[i])
        for i, w in enumerate((wk, wv, wq, wc, wi, wb))
    ]
    for load in loads:
        load.start()
    wa_rows = wa.shape[0]
    half_rows = wa_rows // 2

    def shard(index):
        return pl.ds(pl.multiple_of(index * wa_rows, wa_rows), wa_rows)

    w_part = half_rows // W_PARTS

    def part_of(index, which, c):
        begin = index * wa_rows + which * half_rows + c * w_part
        return pl.ds(pl.multiple_of(begin, w_part), w_part)

    load_wa = pltpu.make_async_copy(wa, wfull.at[shard(t)], wsem.at[6])
    load_wo = pltpu.make_async_copy(wo, wobuf, wsem.at[7])
    load_wa.start()
    load_wo.start()

    def block_at(index):
        return pl.ds(pl.multiple_of(index * own, own), own)

    phase("norm")
    x = x_ref[...].astype(jnp.float32)
    held[block_at(t), :] = (rms_scale(x) * gain_ref[...]).astype(jnp.bfloat16)
    for row, ref in ((0, kg_ref), (1, qg_ref)):
        for h in range(heads):
            for m in range(2):
                at = (h * 2 + m) * comp
                gains[row : row + 1, at : at + comp] = ref[m : m + 1, :]

    phase("barrier")
    barrier = pltpu.get_barrier_semaphore()

    def hello(where):
        pl.semaphore_signal(barrier, inc=1, device_id=where, device_id_type=MESH)

    for peer in (near, away, diag):
        hello({"tp": peer})
    for peer in (t, near, away, diag):
        hello({"sp": mate, "tp": peer})

    plain_up = level < levels - 2
    plain_down = has_down & (level < levels - 1)

    @pl.when(plain_up)
    def _():
        hello({"sp": s + 2})

    @pl.when(plain_down)
    def _():
        hello({"sp": s - 2})

    @pl.when(high_pair == 1)
    def _():
        for which in range(2):
            for peer in range(tp):
                hello({"sp": (cross_sp // 2) * 2 + which, "tp": peer})

    @pl.when((side == 1) & has_up)
    def _():
        hello({"sp": s + 1})

    @pl.when((side == 0) & has_down)
    def _():
        hello({"sp": s - 1})

    expected = 7 + as_int(plain_up) + as_int(plain_down) + 2 * tp * high_pair
    pl.semaphore_wait(barrier, expected + side * ups + (1 - side) * downs)

    phase("defs")
    part = own // CHUNKS

    def chunk_at(index, c):
        return pl.ds(pl.multiple_of(index * own + c * part, part), part)

    def far_copy(c):
        spot = held.at[chunk_at(t, c)]
        return remote(spot, spot, far_send.at[c], far_recv.at[c], {"tp": away})

    def forward(c):
        spot = held.at[chunk_at(away, c)]
        return remote(spot, spot, fwd_send.at[c], fwd_recv.at[c], {"tp": near})

    far_copies = [far_copy(c) for c in range(CHUNKS)]
    forwards = [forward(c) for c in range(CHUNKS)]
    mine = held.at[block_at(t)]
    near_copy = remote(mine, mine, near_sem.at[0], near_sem.at[1], {"tp": near})
    near_copy.start()
    for copy in far_copies:
        copy.start()
    for h in range(heads):
        lamb[0, h] = jnp.full(lamb.shape[2:], lam_ref[h], jnp.float32)
    lam_copy = remote(lamb.at[0], lamb.at[1], lam_sem.at[0], lam_sem.at[1], {"tp": near})
    lam_copy.start()

    w_near = remote(wa, wfull.at[shard(t)], w_send.at[0], w_recv.at[0], {"tp": near})
    def w_far(c):
        return remote(
            wa.at[pl.ds(pl.multiple_of(side * half_rows + c * w_part, w_part), w_part)],
            wfull.at[part_of(t, side, c)], w_send.at[1 + c], w_recv.at[1 + c], {"tp": away},
        )

    def w_side(c):
        spot = wfull.at[part_of(away, side, c)]
        return remote(spot, spot, w_send.at[3 + c], w_recv.at[3 + c], mate_id)

    def w_pass(which, kind, c):
        spot = wfull.at[part_of(away, which, c)]
        slot = 5 + 2 * kind + c
        return remote(spot, spot, w_send.at[slot], w_recv.at[slot], {"tp": near})

    def w_spread(c):
        w_far(c).wait_recv()
        w_side(c).start()
        w_pass(side, 0, c).start()

    def slot_of(lev, pair):
        return lev * 2 + pair

    def group_of(lev, pair, which):
        return (lev * 2 + pair) * 2 + which

    def side_rows(which):
        return pl.ds(pl.multiple_of(which * half, half), half)

    def up_copy(lev, pair, which):
        g = group_of(lev, pair, which)
        return remote(
            kvb.at[0, slot_of(lev, pair), side_rows(which)],
            kvb.at[aside, slot_of(lev, pair), side_rows(which)],
            up_send.at[g], kv_recv.at[aside * groups + g], up_id,
        )

    def arrived(where, lev, pair, which):
        spot = kvb.at[where, slot_of(lev, pair), side_rows(which)]
        g = group_of(lev, pair, which)
        remote(spot, spot, up_send.at[g], kv_recv.at[where * groups + g], up_id).wait_recv()

    def give_copy(pair):
        return remote(
            give_kv.at[pair], kvb.at[0, slot_of(level, pair), side_rows(side)],
            gk_send.at[pair], kv_recv.at[group_of(level, pair, side)], mate_id,
        )

    def q_rows(which, pair):
        return pl.ds(pl.multiple_of(which * rows + pair * half, half), half)

    def giveq_copy(pair):
        return remote(
            give_q.at[pair], qb.at[0, q_rows(side, pair)], gq_send.at[pair], q_recv.at[pair],
            mate_id,
        )

    def swap_q(which, pair):
        index = which * 2 + pair
        return remote(
            qb.at[0, q_rows(which, pair)], qb.at[1, q_rows(which, pair)],
            qs_send.at[index], qs_recv.at[index], cross_id,
        )

    def pass_q(which, pair):
        @pl.when(swaps)
        def _():
            swap_q(which, pair).start()

    def split(values):
        low, high = values[:, :head_cols], values[:, head_cols:]
        return jnp.where(side == 0, low, high), jnp.where(side == 0, high, low)

    def pair_rows(pair):
        return pl.ds(pl.multiple_of(pair * half, half), half)

    def scaled(block, i, gain_row, factor):
        res = jnp.dot(block, wbuf[i], preferred_element_type=jnp.float32).astype(jnp.bfloat16)
        wide = res.astype(jnp.float32)
        return (wide * group_scale(wide, comp) * (gains[gain_row : gain_row + 1] * factor)).astype(
            jnp.bfloat16
        )

    def project_kv(pair):
        block = held[pair_rows(pair)]
        slot = slot_of(level, pair)
        for i in range(2):
            if i == 0:
                res = scaled(block, 0, 0, 1.0)
            else:
                res = jnp.dot(block, wbuf[1], preferred_element_type=jnp.float32).astype(
                    jnp.bfloat16
                )
            keep, give = split(res)
            cols = slice(i * head_cols, (i + 1) * head_cols)
            kvb[0, slot, side_rows(side), cols] = keep
            give_kv[pair, :, cols] = give

        give_copy(pair).start()

        @pl.when(sends_own)
        def _():
            up_copy(level, pair, side).start()

    def project_q(pair):
        block = held[pair_rows(pair)]
        keep, give = split(scaled(block, 2, 1, comp ** (-0.5)))
        qb[0, q_rows(side, pair)] = keep
        give_q[pair] = give
        giveq_copy(pair).start()
        pass_q(side, pair)

    def project_conv(pair):
        block = held[pair_rows(pair)]
        for i in range(3):
            cbuf[pair_rows(pair), i * channels : (i + 1) * channels] = jnp.dot(
                block, wbuf[3 + i], preferred_element_type=jnp.float32
            ).astype(jnp.bfloat16)

    def await_mate(pair):
        arrived(0, level, pair, 1 - side)

        @pl.when(sends_own)
        def _():
            up_copy(level, pair, 1 - side).start()

    def relay(j, pair):
        for which in (side, 1 - side):
            arrived(0, level - j, pair, which)
            up_copy(level - j, pair, which).start()

    queries = 2 * rows
    tile = min(TILE, half)

    def prepare(phase_index, pair):
        for which in range(2):
            @pl.when(swaps)
            def _():
                swap_q(which, pair).wait_recv()

            lane = lax.broadcasted_iota(jnp.int32, (half, both), 1)
            for h in range(per):
                q = qb[swapped, q_rows(which, pair), h * both : (h + 1) * both]
                zero = jnp.zeros_like(q)
                at = phase_index * rows + which * half
                qpad[h, at : at + half] = jnp.where(lane < comp, q, zero)
                qpad[h, queries + at : queries + at + half] = jnp.where(lane < comp, zero, q)

    def run_tiles(work):
        def score(item):
            h, keys, values, at, mask = item
            return lax.dot_general(
                keys(), qpad[h, at], (((1,), (1,)), ((), ())), preferred_element_type=jnp.float32
            )

        def finish(item):
            h, values, at, p, factor = item
            acc[h, :, at] = acc[h, :, at] * factor + jnp.dot(
                values(), p, preferred_element_type=jnp.float32
            )

        ahead = [score(item) for item in work[:DEPTH]]
        late = None
        for index, (h, keys, values, at, mask) in enumerate(work):
            scores = ahead.pop(0)
            if index + DEPTH < len(work):
                ahead.append(score(work[index + DEPTH]))
            if mask is not None:
                kpos = lax.broadcasted_iota(jnp.int32, scores.shape, 0)
                qpos = mask + lax.broadcasted_iota(jnp.int32, scores.shape, 1)
                scores = jnp.where(kpos <= qpos, scores, -1e30)
            old = top[h : h + 1, at]
            new = jnp.maximum(old, jnp.max(scores, axis=0, keepdims=True))
            p = jnp.exp(scores - new)
            factor = jnp.exp(old - new)
            top[h : h + 1, at] = new
            total[h : h + 1, at] = total[h : h + 1, at] * factor + jnp.sum(
                p, axis=0, keepdims=True
            )
            if late is not None:
                finish(late)
            late = (h, values, at, p.astype(jnp.bfloat16), factor)
        finish(late)

    def key_part(slot, h, begin, size):
        return lambda: kvb[swapped, slot, begin : begin + size, h * both : (h + 1) * both]

    def value_part(where, h, begin, size):
        return lambda: vt[where, h, :, begin : begin + size]

    def turn_values(slot, where):
        for h in range(per):
            cols = slice(head_cols + h * vsize, head_cols + (h + 1) * vsize)
            vt[where, h] = kvb[swapped, slot, :, cols].T

    def taken(lev, pair):
        @pl.when(swaps)
        def _():
            for which in range(2):
                arrived(1, lev, pair, which)

    def absorb(j, pair, phases):
        lev = job_level - j
        if 0 in phases:
            taken(lev, pair)
        slot = slot_of(lev, pair)
        turn_values(slot, 0)
        run_tiles(
            [
                (
                    h, key_part(slot, h, which * half, half),
                    value_part(0, h, which * half, half), slice(start, start + tile), None,
                )
                for h in range(per)
                for ph in phases
                for m in range(2)
                for start in range(
                    m * queries + ph * rows, m * queries + (ph + 1) * rows, tile
                )
                for which in range(2)
            ]
        )

    pairs = (first, second)

    def diag_work(blocks):
        work = []
        for h in range(per):
            for q_ph, q_side, k_ph, k_side in blocks:
                same = q_ph == k_ph and q_side == k_side
                slot = slot_of(job_level, pairs[k_ph])
                for m in range(2):
                    base = m * queries + q_ph * rows + q_side * half
                    for offset in range(0, half, tile):
                        size = offset + tile if same else half
                        work.append(
                            (
                                h, key_part(slot, h, k_side * half, size),
                                value_part(1 + k_ph, h, k_side * half, size),
                                slice(base + offset, base + offset + tile),
                                offset if same else None,
                            )
                        )
        return work

    def diag_ready(ph):
        taken(job_level, pairs[ph])
        turn_values(slot_of(job_level, pairs[ph]), 1 + ph)

    phase("wait_kv_weights")
    loads[0].wait()
    loads[1].wait()
    phase("wait_near")
    near_copy.wait_recv()
    phase("kv_first")
    project_kv(first)
    w_near.start()
    phase("q_first")
    loads[2].wait()
    project_q(first)
    phase("conv_first")
    for load in loads[3:]:
        load.wait()
    project_conv(first)
    tail_copy = remote(
        cbuf.at[pl.ds(rows - EDGE, EDGE), pl.ds(0, 2 * channels)], tail,
        tail_sem.at[0], tail_sem.at[1], {"sp": jnp.minimum(s + 1, sp - 1)},
    )

    @pl.when((s < sp - 1) & (first == 1))
    def _():
        tail_copy.start()

    phase("mate_first")
    await_mate(first)

    phase("below_first")
    @pl.when(has_down & relays)
    def _():
        relay(1, first)

    giveq_copy(first).wait_recv()
    pass_q(1 - side, first)
    phase("early")
    top[...] = jnp.full_like(top, -1e30)
    total[...] = jnp.zeros_like(total)
    acc[...] = jnp.zeros_like(acc)

    def early():
        prepare(0, first)
        diag_ready(0)
        run_tiles(diag_work([(0, 0, 0, 0), (0, 1, 0, 0), (0, 1, 0, 1)]))

    for c in range(CHUNKS - 1):
        far_copies[c].wait_recv()
        forwards[c].start()

    @pl.when(jnp.logical_not(swaps))
    def _():
        early()

    phase("far_wait")
    far_copies[CHUNKS - 1].wait_recv()
    forwards[CHUNKS - 1].start()
    for c in range(W_PARTS):
        w_far(c).start()
    for copy in forwards:
        copy.wait_recv()
    phase("kv_second")
    project_kv(second)
    phase("q_second")
    project_q(second)
    phase("below_first2")

    @pl.when((level > 1) & relays)
    def _():
        relay(2, first)

    phase("conv_second")
    project_conv(second)

    @pl.when((s < sp - 1) & (first == 0))
    def _():
        tail_copy.start()

    phase("early2")

    @pl.when(swaps)
    def _():
        early()

    @pl.when(relays)
    def _():
        @pl.loop(1, jnp.minimum(job_level, 2) + 1)
        def _(j):
            absorb(j, first, (0,))

    phase("mate_second")
    await_mate(second)

    phase("qpad")
    giveq_copy(second).wait_recv()
    pass_q(1 - side, second)
    phase("w_first")
    w_spread(0)
    phase("conv")
    def product(ref):
        gate = ref[:, :channels].astype(jnp.float32)
        other = ref[:, channels : 2 * channels].astype(jnp.float32)
        return (gate * other).astype(jnp.bfloat16).astype(jnp.float32)

    padded[EDGE:] = product(cbuf)

    @pl.when(s > 0)
    def _():
        tail_copy.wait_recv()
        padded[:EDGE] = product(tail)

    @pl.when(s == 0)
    def _():
        padded[:EDGE] = jnp.zeros((EDGE, channels), jnp.float32)

    count = taps_ref.shape[0]
    conv = jnp.zeros((rows, channels), jnp.float32)
    for tap in range(count):
        begin = EDGE - count + 1 + tap
        conv = conv + taps_ref[tap : tap + 1] * padded[begin : begin + rows]
    gated = cbuf[:, 2 * channels :].astype(jnp.float32) * conv
    cvout[...] = (gated * group_scale(gated, GROUP) * cgain_ref[...]).astype(jnp.bfloat16)
    load_wo.wait()

    def partial(target):
        return jnp.dot(cvout[block_at(target), :], wobuf[...], preferred_element_type=jnp.float32)

    cross_copy = remote(cross, cross_in, cross_send, cross_recv, {"tp": near})
    fin_copy = remote(fin, fin_in, fin_send, fin_recv, {"tp": near})
    far_sum = remote(far, far_in, fs_send, fs_recv, {"tp": away})
    phase("partial")
    cross[...] = partial(diag).astype(jnp.bfloat16)
    cross_copy.start()
    fin[...] = partial(near).astype(jnp.bfloat16)
    fin_copy.start()
    out_ref[...] = partial(t)
    phase("relay_second")

    @pl.when(has_down & relays)
    def _():
        relay(1, second)

    phase("toward")
    toward = partial(away)
    cross_copy.wait_recv()
    far[...] = (toward + cross_in[...].astype(jnp.float32)).astype(jnp.bfloat16)
    far_sum.start()
    phase("w_far")
    w_spread(1)
    phase("q_late")
    prepare(1, second)
    phase("near_loop")

    @pl.loop(1, job_level + 1)
    def _(j):
        @pl.when((j > 1) & (j < level) & relays)
        def _():
            relay(j + 1, first)

        @pl.when((j == job_level) & (level > 1) & (is_top == 0))
        def _():
            relay(2, second)

        @pl.when((j > 2) | jnp.logical_not(relays))
        def _():
            absorb(j, first, (0,))

        absorb(j, first, (1,))

    phase("diag")
    diag_ready(1)
    run_tiles(
        diag_work([(1, 0, 1, 0), (1, 1, 1, 0), (1, 1, 1, 1), (1, 1, 0, 0), (0, 1, 1, 0)])
    )

    @pl.when(first == 1)
    def _():
        run_tiles(diag_work([(0, 0, 1, 0), (0, 1, 1, 1)]))

    @pl.when(first == 0)
    def _():
        run_tiles(diag_work([(1, 0, 0, 0), (1, 1, 0, 1)]))

    @pl.when((level > 1) & (is_top * odd == 1))
    def _():
        relay(2, second)

    phase("far_loop")

    @pl.loop(1, job_level + 1)
    def _(j):
        absorb(j, second, (0, 1))

        @pl.when((j > 1) & (j < level) & relays)
        def _():
            relay(j + 1, second)

    phase("w_side")
    for c in range(W_PARTS):
        w_side(c).wait_recv()
        w_pass(1 - side, 1, c).start()

    phase("finalize")
    lam_copy.wait_recv()
    for h in range(per):
        inverse = 1.0 / total[h : h + 1]
        mapped = acc[h] * inverse
        factor = lamb[swapped, side * per + h][0:1, 0:1]
        attn = mapped[:, :queries] - factor * mapped[:, queries:]
        scale = lax.rsqrt(jnp.mean(attn * attn, axis=0, keepdims=True) + eps)
        result = ((attn * scale).T * sub_ref[...]).astype(jnp.bfloat16)
        for ph in range(2):
            for which in range(2):
                at = ph * rows + which * half
                obuf[q_rows(which, pairs[ph]), h * vsize : (h + 1) * vsize] = result[
                    at : at + half
                ]
        logs = top[h : h + 1] + jnp.log(total[h : h + 1])
        for m in range(2):
            ordered = []
            for which in range(2):
                at = m * queries + which * half
                early, late = logs[:, at : at + half], logs[:, at + rows : at + rows + half]
                ordered.append(
                    jnp.concatenate(
                        [
                            jnp.where(first == 0, early, late),
                            jnp.where(first == 0, late, early),
                        ],
                        axis=1,
                    )
                )
            low, high = ordered
            lout[0, h, m : m + 1, :] = jnp.where(side == 0, low, high)
            lout[1, h, m : m + 1, :] = jnp.where(side == 0, high, low)

    phase("send_o")
    me8 = job_tp * 2 + side

    def piece_rows(which, target):
        return pl.ds(pl.multiple_of(which * rows + target * own, own), own)

    def o_copy(which, target, index):
        return remote(
            obuf.at[piece_rows(which, target)], hin.at[me8], o_send.at[index], o_recv.at[me8],
            {"sp": job_level * 2 + which, "tp": target},
        )

    def o_wait(which, source, index):
        spot = hin.at[source * 2 + which]
        return remote(spot, spot, o_send.at[index], o_recv.at[source * 2 + which], mate_id)

    peers = [(1 - side, diag), (1 - side, away), (side, diag), (side, away)]
    peers += [(1 - side, t), (1 - side, near), (side, near)]
    for index, (which, target) in enumerate(peers):
        o_copy(which, target, index).start()
    def log_copy(index):
        which = side + index - 2 * index * side
        return remote(
            lout.at[index], lin.at[index], log_send.at[index], log_recv.at[index],
            {"sp": job_level * 2 + which, "tp": job_tp},
        )

    log_copy(1).start()

    @pl.when(swaps)
    def _():
        o_copy(side, t, 7).start()
        log_copy(0).start()

    @pl.when(jnp.logical_not(swaps))
    def _():
        hin[me8] = obuf[piece_rows(side, t)]
        for h in range(per):
            log_ref[side * per + h] = lout[0, h]

    phase("conv_sum")
    fin_copy.wait_recv()
    far_sum.wait_recv()
    out_ref[...] += fin_in[...].astype(jnp.float32) + far_in[...].astype(jnp.float32)
    phase("w_wait")
    load_wa.wait()
    w_near.wait_recv()
    for c in range(W_PARTS):
        w_pass(side, 0, c).wait_recv()
        w_pass(1 - side, 1, c).wait_recv()
    phase("o_wait")
    for index, (which, source) in enumerate(peers):
        o_wait(which, source, index).wait_recv()

    @pl.when(swaps)
    def _():
        o_wait(side, t, 7).wait_recv()
        log_copy(0).wait_recv()
        for h in range(per):
            log_ref[side * per + h] = lin[0, h]

    phase("last_dot")
    lhs = jnp.concatenate([hin[i] for i in range(2 * tp)], axis=1)
    out_ref[...] += jnp.dot(lhs, wfull[...], preferred_element_type=jnp.float32)
    phase("log")
    log_copy(1).wait_recv()
    for h in range(per):
        log_ref[(1 - side) * per + h] = lin[1, h]

    phase("sends")
    near_copy.wait_send()
    for copy in far_copies + forwards:
        copy.wait_send()
    for pair in range(2):
        give_copy(pair).wait_send()
        giveq_copy(pair).wait_send()
    w_near.wait_send()
    for c in range(W_PARTS):
        for copy in (w_far(c), w_side(c), w_pass(side, 0, c), w_pass(1 - side, 1, c)):
            copy.wait_send()
    for copy in (cross_copy, fin_copy, far_sum, log_copy(1), lam_copy):
        copy.wait_send()
    for index, (which, target) in enumerate(peers):
        o_copy(which, target, index).wait_send()

    @pl.when(swaps)
    def _():
        o_copy(side, t, 7).wait_send()
        log_copy(0).wait_send()
        for which in range(2):
            for pair in range(2):
                swap_q(which, pair).wait_send()

    @pl.loop(is_top * (1 - odd) * level, level + 1 - is_top * odd)
    def _(lev):
        for pair in range(2):
            for which in range(2):
                up_copy(lev, pair, which).wait_send()

    @pl.when(s < sp - 1)
    def _():
        tail_copy.wait_send()

    phase(None)


def phase(name):
    pass


def vmem():
    return pl.BlockSpec(memory_space=pltpu.VMEM)


def on_device(
    inputs, norm_gain, w_query, w_key, w_value, query_gain, key_gain, lambdas, sub_gain,
    w_gate_b, w_gate_c, w_conv_in, conv_taps, conv_gain, w_out_att, w_out_conv,
):
    heads = lambdas.shape[0]
    comp = query_gain.shape[1]
    vsize = sub_gain.shape[0]
    channels = conv_gain.shape[0]
    own, width = inputs.shape
    tp = lax.axis_size("tp")
    sp = lax.axis_size("sp")
    rows = own * tp
    half = rows // 2
    qcols = heads * 2 * comp
    mine = qcols // 2
    per = heads // 2
    dma = pltpu.SemaphoreType.DMA
    bf, f32 = jnp.bfloat16, jnp.float32
    weights = (w_key, w_value, w_query, w_gate_c, w_conv_in, w_gate_b, w_out_att, w_out_conv)
    groups = sp // 2 * 4
    piece = pltpu.VMEM((own, width), bf)
    any_spec = pl.BlockSpec(memory_space=pl.ANY)
    mixed, log_sums = pl.pallas_call(
        functools.partial(layer, sp, tp, comp, heads),
        out_shape=(
            jax.ShapeDtypeStruct((own, width), f32),
            jax.ShapeDtypeStruct((heads, 2, rows), f32),
        ),
        in_specs=[vmem()] * 4 + [pl.BlockSpec(memory_space=pltpu.SMEM)] + [vmem()] * 3
        + [any_spec] * 8,
        out_specs=(vmem(), vmem()),
        scratch_shapes=[
            pltpu.VMEM((rows, width), bf),
            pltpu.VMEM((6, width, qcols), bf),
            pltpu.VMEM((tp * w_out_att.shape[0], width), bf),
            pltpu.VMEM(w_out_conv.shape, bf),
            pltpu.VMEM((8, qcols), f32),
            pltpu.VMEM((2, sp, 2 * half, 2 * mine), bf),
            pltpu.VMEM((3, per, vsize, 2 * half), bf),
            pltpu.VMEM((2, 2 * rows, mine), bf),
            pltpu.VMEM((2, half, 2 * mine), bf),
            pltpu.VMEM((2, half, mine), bf),
            pltpu.VMEM((per, 4 * rows, 2 * comp), bf),
            pltpu.VMEM((per, 4 * rows), f32),
            pltpu.VMEM((per, 4 * rows), f32),
            pltpu.VMEM((per, vsize, 4 * rows), f32),
            pltpu.VMEM((rows, 3 * channels), bf),
            pltpu.VMEM((EDGE, 2 * channels), bf),
            pltpu.VMEM((EDGE + rows, channels), f32),
            pltpu.VMEM((rows, channels), bf),
            pltpu.VMEM((2, heads, 8, 128), f32),
            piece, piece, piece, piece, piece, piece,
            pltpu.VMEM((2 * rows, per * vsize), bf),
            pltpu.VMEM((2 * tp, own, per * vsize), bf),
            pltpu.VMEM((2, per, 2, rows), f32),
            pltpu.VMEM((2, per, 2, rows), f32),
            dma((8,)), dma((2,)), dma((CHUNKS,)), dma((CHUNKS,)), dma((CHUNKS,)), dma((CHUNKS,)),
            dma((groups,)), dma((2 * groups,)), dma((2,)), dma((2,)), dma((2,)), dma((2,)),
            dma((9,)), dma((9,)), dma(()), dma(()), dma(()), dma(()), dma(()), dma(()),
            dma((8,)), dma((2 * tp,)), dma((2,)), dma((2,)), dma((2,)), dma((4,)), dma((4,)),
        ],
        compiler_params=pltpu.CompilerParams(
            collective_id=0, has_side_effects=True, vmem_limit_bytes=VMEM_LIMIT
        ),
        name="layer",
    )(
        inputs, norm_gain[None], query_gain, key_gain, lambdas, sub_gain[None], conv_taps,
        conv_gain[None], *weights,
    )
    return (mixed, log_sums)


def solution(mesh):
    in_specs = (
        P(("sp", "tp"), None),
        P(),
        P(None, "tp"),
        P(None, "tp"),
        P(None, "tp"),
        P(),
        P(),
        P("tp"),
        P(),
        P(None, "tp"),
        P(None, "tp"),
        P(None, "tp"),
        P(None, "tp"),
        P("tp"),
        P("tp", None),
        P("tp", None),
    )
    out_specs = (P(("sp", "tp"), None), P("tp", None, "sp"))
    return jax.shard_map(
        on_device, mesh=mesh, in_specs=in_specs, out_specs=out_specs, check_vma=False
    )
```

```python
import functools

import jax
import jax.numpy as jnp
from jax import lax
from jax.experimental import pallas as pl
from jax.experimental.pallas import tpu as pltpu
from jax.sharding import PartitionSpec as P

GROUP = 64
eps = 1e-06
MESH = pl.DeviceIdType.MESH
VMEM_LIMIT = 62 * 1024 * 1024
CHUNKS = 4
EDGE = 16
TILE = 128
DEPTH = 2
W_PARTS = 2


def rms_scale(values):
    return values * lax.rsqrt(jnp.mean(values * values, axis=-1, keepdims=True) + eps)


def flip(index, bit):
    return index + bit - 2 * bit * lax.rem(index // bit, 2)


def remote(src, dst, send, recv, where):
    return pltpu.make_async_remote_copy(
        src_ref=src, dst_ref=dst, send_sem=send, recv_sem=recv, device_id=where,
        device_id_type=MESH,
    )


def group_scale(values, size):
    lanes = values.shape[1]
    row = lax.broadcasted_iota(jnp.int32, (lanes, lanes), 0) // size
    col = lax.broadcasted_iota(jnp.int32, (lanes, lanes), 1) // size
    ones = jnp.where(row == col, 1.0, 0.0).astype(jnp.bfloat16)
    squares = values * values
    high = squares.astype(jnp.bfloat16)
    low = (squares - high.astype(jnp.float32)).astype(jnp.bfloat16)
    sums = jnp.dot(high, ones, preferred_element_type=jnp.float32) + jnp.dot(
        low, ones, preferred_element_type=jnp.float32
    )
    return lax.rsqrt(sums * (1.0 / size) + eps)


def layer(
    sp, tp, comp, heads,
    x_ref, gain_ref, qg_ref, kg_ref, lam_ref, sub_ref, taps_ref, cgain_ref,
    wk, wv, wq, wc, wi, wb, wa, wo,
    out_hbm, log_hbm, out_ref, log_ref,
    held, wbuf, wfull, wobuf, gains, kvb, vt, qb, give_kv, give_q, qpad, top, total, acc, cbuf, tail,
    padded, cvout, lamb, cross, fin, far, cross_in, fin_in, far_in, obuf, hin, lout, lin,
    wsem, near_sem, far_send, far_recv, fwd_send, fwd_recv, up_send, kv_recv, gk_send, gq_send,
    q_recv, x_recv, tail_sem, w_send, w_recv, cross_send, cross_recv, fin_send, fin_recv, fs_send, fs_recv,
    out_sem, o_send, o_recv, log_send, log_recv, lam_sem, qs_send, qs_recv,
):
    s = lax.axis_index("sp")
    t = lax.axis_index("tp")
    level, side = s // 2, lax.rem(s, 2)
    levels = sp // 2
    mate = level * 2 + 1 - side
    near, away = flip(t, 1), flip(t, 2)
    diag = flip(near, 2)
    first, second = t // 2, 1 - t // 2
    own = x_ref.shape[0]
    rows = own * tp
    half = rows // 2
    head_cols = heads * 2 * comp // 2
    per = heads // 2
    vsize = sub_ref.shape[1]
    both = 2 * comp
    channels = cgain_ref.shape[1]
    has_up, has_down = level < levels - 1, level > 0

    def as_int(flag):
        return flag.astype(jnp.int32)

    ups, downs = as_int(has_up), as_int(has_down)
    mate_id = {"sp": mate}
    odd = lax.rem(t, 2)
    is_top, is_low = as_int(level == levels - 1), as_int(level == levels - 2)
    high_pair = is_top + is_low
    swapped = is_low * odd + is_top * (1 - odd)
    swaps = swapped == 1
    aside = is_low * (1 - odd) + is_top
    job_level = level + is_low * odd - is_top * (1 - odd)
    job_tp = t + swapped * (near - t)
    cross_sp = s + 2 * is_low - 2 * is_top
    cross_id = {"sp": cross_sp, "tp": near}
    up_id = {
        "sp": s + (1 - is_top) * (2 - 2 * is_low * (1 - odd)) - 2 * is_top * (1 - odd),
        "tp": t + aside * (near - t),
    }
    sends_own = is_top * odd == 0
    relays = is_top * (1 - odd) == 0
    groups = sp // 2 * 4

    loads = [
        pltpu.make_async_copy(w, wbuf.at[i], wsem.at[i])
        for i, w in enumerate((wk, wv, wq, wc, wi, wb))
    ]
    for load in loads:
        load.start()
    wa_rows = wa.shape[0]
    half_rows = wa_rows // 2

    def shard(index):
        return pl.ds(pl.multiple_of(index * wa_rows, wa_rows), wa_rows)

    w_part = half_rows // W_PARTS

    def part_of(index, which, c):
        begin = index * wa_rows + which * half_rows + c * w_part
        return pl.ds(pl.multiple_of(begin, w_part), w_part)

    load_wa = pltpu.make_async_copy(wa, wfull.at[shard(t)], wsem.at[6])
    load_wo = pltpu.make_async_copy(wo, wobuf, wsem.at[7])
    load_wa.start()
    load_wo.start()

    def block_at(index):
        return pl.ds(pl.multiple_of(index * own, own), own)

    phase("norm")
    x = x_ref[...].astype(jnp.float32)
    held[block_at(t), :] = (rms_scale(x) * gain_ref[...]).astype(jnp.bfloat16)
    for row, ref in ((0, kg_ref), (1, qg_ref)):
        for h in range(heads):
            for m in range(2):
                at = (h * 2 + m) * comp
                gains[row : row + 1, at : at + comp] = ref[m : m + 1, :]

    phase("barrier")
    barrier = pltpu.get_barrier_semaphore()

    def hello(where):
        pl.semaphore_signal(barrier, inc=1, device_id=where, device_id_type=MESH)

    for peer in (near, away, diag):
        hello({"tp": peer})
    for peer in (t, near, away, diag):
        hello({"sp": mate, "tp": peer})

    plain_up = level < levels - 2
    plain_down = has_down & (level < levels - 1)

    @pl.when(plain_up)
    def _():
        hello({"sp": s + 2})

    @pl.when(plain_down)
    def _():
        hello({"sp": s - 2})

    @pl.when(high_pair == 1)
    def _():
        for which in range(2):
            for peer in range(tp):
                hello({"sp": (cross_sp // 2) * 2 + which, "tp": peer})

    @pl.when((side == 1) & has_up)
    def _():
        hello({"sp": s + 1})

    @pl.when((side == 0) & has_down)
    def _():
        hello({"sp": s - 1})

    expected = 7 + as_int(plain_up) + as_int(plain_down) + 2 * tp * high_pair
    pl.semaphore_wait(barrier, expected + side * ups + (1 - side) * downs)

    phase("defs")
    part = own // CHUNKS

    def chunk_at(index, c):
        return pl.ds(pl.multiple_of(index * own + c * part, part), part)

    def far_copy(c):
        spot = held.at[chunk_at(t, c)]
        return remote(spot, spot, far_send.at[c], far_recv.at[c], {"tp": away})

    def forward(c):
        spot = held.at[chunk_at(away, c)]
        return remote(spot, spot, fwd_send.at[c], fwd_recv.at[c], {"tp": near})

    far_copies = [far_copy(c) for c in range(CHUNKS)]
    forwards = [forward(c) for c in range(CHUNKS)]
    mine = held.at[block_at(t)]
    near_copy = remote(mine, mine, near_sem.at[0], near_sem.at[1], {"tp": near})
    near_copy.start()
    for copy in far_copies:
        copy.start()
    for h in range(heads):
        lamb[0, h] = jnp.full(lamb.shape[2:], lam_ref[h], jnp.float32)
    lam_copy = remote(lamb.at[0], lamb.at[1], lam_sem.at[0], lam_sem.at[1], {"tp": near})
    lam_copy.start()

    w_near = remote(wa, wfull.at[shard(t)], w_send.at[0], w_recv.at[0], {"tp": near})
    def w_far(c):
        return remote(
            wa.at[pl.ds(pl.multiple_of(side * half_rows + c * w_part, w_part), w_part)],
            wfull.at[part_of(t, side, c)], w_send.at[1 + c], w_recv.at[1 + c], {"tp": away},
        )

    def w_side(c):
        spot = wfull.at[part_of(away, side, c)]
        return remote(spot, spot, w_send.at[3 + c], w_recv.at[3 + c], mate_id)

    def w_pass(which, kind, c):
        spot = wfull.at[part_of(away, which, c)]
        slot = 5 + 2 * kind + c
        return remote(spot, spot, w_send.at[slot], w_recv.at[slot], {"tp": near})

    def w_spread(c):
        w_far(c).wait_recv()
        w_side(c).start()
        w_pass(side, 0, c).start()

    def slot_of(lev, pair):
        return lev * 2 + pair

    def group_of(lev, pair, which):
        return (lev * 2 + pair) * 2 + which

    def side_rows(which):
        return pl.ds(pl.multiple_of(which * half, half), half)

    def up_copy(lev, pair, which):
        g = group_of(lev, pair, which)
        return remote(
            kvb.at[0, slot_of(lev, pair), side_rows(which)],
            kvb.at[aside, slot_of(lev, pair), side_rows(which)],
            up_send.at[g], kv_recv.at[aside * groups + g], up_id,
        )

    def arrived(where, lev, pair, which):
        spot = kvb.at[where, slot_of(lev, pair), side_rows(which)]
        g = group_of(lev, pair, which)
        remote(spot, spot, up_send.at[g], kv_recv.at[where * groups + g], up_id).wait_recv()

    sub = own // 2

    def part_span(base, part):
        if part is None:
            return pl.ds(pl.multiple_of(base, half), half)
        return pl.ds(pl.multiple_of(base + part * own, own), own)

    def give_copy(pair, part):
        index = 0 if part is None else 1 + part
        arrival = kv_recv.at[group_of(level, pair, side)] if part is None else x_recv.at[part]
        return remote(
            give_kv.at[pair, part_span(0, part)],
            kvb.at[0, slot_of(level, pair), part_span(side * half, part)],
            gk_send.at[index], arrival, mate_id,
        )

    def q_rows(which, pair):
        return pl.ds(pl.multiple_of(which * rows + pair * half, half), half)

    def giveq_copy(pair, part):
        index = 0 if part is None else 1 + part
        return remote(
            give_q.at[pair, part_span(0, part)],
            qb.at[0, part_span(side * rows + pair * half, part)],
            gq_send.at[index], q_recv.at[index], mate_id,
        )

    def swap_q(which, pair):
        index = which * 2 + pair
        return remote(
            qb.at[0, q_rows(which, pair)], qb.at[1, q_rows(which, pair)],
            qs_send.at[index], qs_recv.at[index], cross_id,
        )

    def pass_q(which, pair):
        @pl.when(swaps)
        def _():
            swap_q(which, pair).start()

    def split(values):
        low, high = values[:, :head_cols], values[:, head_cols:]
        return jnp.where(side == 0, low, high), jnp.where(side == 0, high, low)

    def pair_rows(pair):
        return pl.ds(pl.multiple_of(pair * half, half), half)

    def scaled(block, i, gain_row, factor):
        res = jnp.dot(block, wbuf[i], preferred_element_type=jnp.float32).astype(jnp.bfloat16)
        wide = res.astype(jnp.float32)
        return (wide * group_scale(wide, comp) * (gains[gain_row : gain_row + 1] * factor)).astype(
            jnp.bfloat16
        )

    def source(pair, part):
        if part is None:
            return held[pair_rows(pair)]
        return jnp.concatenate(
            [
                held[pl.ds(pl.multiple_of(pair * half + b * own + part * sub, sub), sub)]
                for b in range(2)
            ],
            axis=0,
        )

    def project_kv(pair, part=None):
        block = source(pair, part)
        slot = slot_of(level, pair)
        for i in range(2):
            if i == 0:
                res = scaled(block, 0, 0, 1.0)
            else:
                res = jnp.dot(block, wbuf[1], preferred_element_type=jnp.float32).astype(
                    jnp.bfloat16
                )
            keep, give = split(res)
            cols = slice(i * head_cols, (i + 1) * head_cols)
            kvb[0, slot, part_span(side * half, part), cols] = keep
            give_kv[pair, part_span(0, part), cols] = give

        give_copy(pair, part).start()
        if part != 0:
            @pl.when(sends_own)
            def _():
                up_copy(level, pair, side).start()

    def project_q(pair, part=None):
        block = source(pair, part)
        keep, give = split(scaled(block, 2, 1, comp ** (-0.5)))
        qb[0, part_span(side * rows + pair * half, part)] = keep
        give_q[pair, part_span(0, part)] = give
        giveq_copy(pair, part).start()
        if part != 0:
            pass_q(side, pair)

    def project_conv(pair, part=None):
        block = source(pair, part)
        for i in range(3):
            res = jnp.dot(block, wbuf[3 + i], preferred_element_type=jnp.float32).astype(
                jnp.bfloat16
            )
            cols = slice(i * channels, (i + 1) * channels)
            if part is None:
                cbuf[pair_rows(pair), cols] = res
            else:
                for b in range(2):
                    begin = pl.multiple_of(pair * half + b * own + part * sub, sub)
                    cbuf[pl.ds(begin, sub), cols] = res[b * sub : (b + 1) * sub]

    def await_mate(pair, parts):
        if parts is None:
            arrived(0, level, pair, 1 - side)
        else:
            for part in parts:
                give_copy(pair, part).wait_recv()

        @pl.when(sends_own)
        def _():
            up_copy(level, pair, 1 - side).start()

    def relay(j, pair, sides=(side, 1 - side)):
        for which in sides:
            arrived(0, level - j, pair, which)
            up_copy(level - j, pair, which).start()

    queries = 2 * rows
    tile = min(TILE, half)

    def prepare(phase_index, pair):
        for which in range(2):
            @pl.when(swaps)
            def _():
                swap_q(which, pair).wait_recv()

            lane = lax.broadcasted_iota(jnp.int32, (half, both), 1)
            for h in range(per):
                q = qb[swapped, q_rows(which, pair), h * both : (h + 1) * both]
                zero = jnp.zeros_like(q)
                at = phase_index * rows + which * half
                qpad[h, at : at + half] = jnp.where(lane < comp, q, zero)
                qpad[h, queries + at : queries + at + half] = jnp.where(lane < comp, zero, q)

    def position(index):
        low = index % own
        return low // sub * own + index // own * sub + low % sub

    def run_tiles(work):
        def score(item):
            h, keys, values, at, mask = item
            return lax.dot_general(
                keys(), qpad[h, at], (((1,), (1,)), ((), ())), preferred_element_type=jnp.float32
            )

        def finish(item):
            h, values, at, p, factor = item
            acc[h, :, at] = acc[h, :, at] * factor + jnp.dot(
                values(), p, preferred_element_type=jnp.float32
            )

        ahead = [score(item) for item in work[:DEPTH]]
        late = None
        for index, (h, keys, values, at, mask) in enumerate(work):
            scores = ahead.pop(0)
            if index + DEPTH < len(work):
                ahead.append(score(work[index + DEPTH]))
            if mask is not None:
                kpos = lax.broadcasted_iota(jnp.int32, scores.shape, 0)
                qpos = mask[0] + lax.broadcasted_iota(jnp.int32, scores.shape, 1)
                if mask[1]:
                    kpos, qpos = position(kpos), position(qpos)
                scores = jnp.where(kpos <= qpos, scores, -1e30)
            old = top[h : h + 1, at]
            new = jnp.maximum(old, jnp.max(scores, axis=0, keepdims=True))
            p = jnp.exp(scores - new)
            factor = jnp.exp(old - new)
            top[h : h + 1, at] = new
            total[h : h + 1, at] = total[h : h + 1, at] * factor + jnp.sum(
                p, axis=0, keepdims=True
            )
            if late is not None:
                finish(late)
            late = (h, values, at, p.astype(jnp.bfloat16), factor)
        finish(late)

    def key_part(slot, h, begin, size):
        return lambda: kvb[swapped, slot, begin : begin + size, h * both : (h + 1) * both]

    def value_part(where, h, begin, size):
        return lambda: vt[where, h, :, begin : begin + size]

    def turn_values(slot, where):
        for h in range(per):
            cols = slice(head_cols + h * vsize, head_cols + (h + 1) * vsize)
            vt[where, h] = kvb[swapped, slot, :, cols].T

    def taken(lev, pair):
        @pl.when(swaps)
        def _():
            for which in range(2):
                arrived(1, lev, pair, which)

    def absorb(j, pair, phases, take):
        lev = job_level - j
        if take:
            taken(lev, pair)
        slot = slot_of(lev, pair)
        turn_values(slot, 0)
        run_tiles(
            [
                (
                    h, key_part(slot, h, which * half, half),
                    value_part(0, h, which * half, half), slice(start, start + tile), None,
                )
                for h in range(per)
                for ph in phases
                for m in range(2)
                for start in range(
                    m * queries + ph * rows, m * queries + (ph + 1) * rows, tile
                )
                for which in range(2)
            ]
        )

    pairs = (first, second)

    def diag_work(blocks):
        work = []
        for h in range(per):
            for q_ph, q_side, k_ph, k_side in blocks:
                same = q_ph == k_ph and q_side == k_side
                slot = slot_of(job_level, pairs[k_ph])
                for m in range(2):
                    base = m * queries + q_ph * rows + q_side * half
                    for offset in range(0, half, tile):
                        size = offset + tile if same and q_ph == 0 else half
                        work.append(
                            (
                                h, key_part(slot, h, k_side * half, size),
                                value_part(1 + k_ph, h, k_side * half, size),
                                slice(base + offset, base + offset + tile),
                                (offset, q_ph == 1) if same else None,
                            )
                        )
        return work

    def diag_ready(ph):
        taken(job_level, pairs[ph])
        turn_values(slot_of(job_level, pairs[ph]), 1 + ph)

    phase("wait_kv_weights")
    loads[0].wait()
    loads[1].wait()
    phase("wait_near")
    near_copy.wait_recv()
    phase("kv_first")
    project_kv(first)
    w_near.start()
    phase("q_first")
    loads[2].wait()
    project_q(first)
    phase("conv_first")
    for load in loads[3:]:
        load.wait()
    project_conv(first)
    tail_copy = remote(
        cbuf.at[pl.ds(rows - EDGE, EDGE), pl.ds(0, 2 * channels)], tail,
        tail_sem.at[0], tail_sem.at[1], {"sp": jnp.minimum(s + 1, sp - 1)},
    )

    @pl.when((s < sp - 1) & (first == 1))
    def _():
        tail_copy.start()

    phase("mate_first")
    await_mate(first, None)
    phase("part_a")
    for c in range(CHUNKS // 2):
        far_copies[c].wait_recv()
        forwards[c].start()
    for c in range(CHUNKS // 2):
        forwards[c].wait_recv()
    project_kv(second, 0)
    project_q(second, 0)
    project_conv(second, 0)

    phase("below_first")
    @pl.when(has_down & relays)
    def _():
        relay(1, first)

    giveq_copy(first, None).wait_recv()
    pass_q(1 - side, first)
    phase("early")
    top[...] = jnp.full_like(top, -1e30)
    total[...] = jnp.zeros_like(total)
    acc[...] = jnp.zeros_like(acc)

    def early():
        prepare(0, first)
        diag_ready(0)
        run_tiles(diag_work([(0, 0, 0, 0), (0, 1, 0, 0), (0, 1, 0, 1)]))

    for c in range(CHUNKS // 2, CHUNKS - 1):
        far_copies[c].wait_recv()
        forwards[c].start()

    for c in range(W_PARTS):
        w_far(c).start()

    @pl.when(jnp.logical_not(swaps))
    def _():
        early()

    phase("far_wait")
    far_copies[CHUNKS - 1].wait_recv()
    forwards[CHUNKS - 1].start()
    for copy in forwards[CHUNKS // 2 :]:
        copy.wait_recv()
    phase("kv_second")
    project_kv(second, 1)
    phase("q_second")
    project_q(second, 1)
    phase("conv_second")
    project_conv(second, 1)

    @pl.when((s < sp - 1) & (first == 0))
    def _():
        tail_copy.start()

    phase("below_first2")

    @pl.when((level > 1) & relays)
    def _():
        relay(2, first)

    phase("early2a")

    @pl.when(swaps & relays)
    def _():
        early()

    @pl.when(jnp.logical_not(swaps) & (job_level > 0))
    def _():
        absorb(1, first, (0,), True)

    phase("mate_second")
    await_mate(second, (0, 1))

    @pl.when(swaps)
    def _():
        for part in range(2):
            giveq_copy(second, part).wait_recv()
        swap_q(1 - side, second).start()

    phase("early2")

    @pl.when(jnp.logical_not(relays))
    def _():
        early()

    @pl.when(relays)
    def _():
        @pl.loop(2 - swapped, jnp.minimum(job_level, 2) + 1)
        def _(j):
            absorb(j, first, (0,), True)

    @pl.when(jnp.logical_not(swaps))
    def _():
        for part in range(2):
            giveq_copy(second, part).wait_recv()

    @pl.when(has_down & relays)
    def _():
        relay(1, second, (side,))

    phase("w_first")
    w_spread(0)
    phase("conv")
    def product(ref):
        gate = ref[:, :channels].astype(jnp.float32)
        other = ref[:, channels : 2 * channels].astype(jnp.float32)
        return (gate * other).astype(jnp.bfloat16).astype(jnp.float32)

    padded[EDGE:] = product(cbuf)

    @pl.when(s > 0)
    def _():
        tail_copy.wait_recv()
        padded[:EDGE] = product(tail)

    @pl.when(s == 0)
    def _():
        padded[:EDGE] = jnp.zeros((EDGE, channels), jnp.float32)

    count = taps_ref.shape[0]
    conv = jnp.zeros((rows, channels), jnp.float32)
    for tap in range(count):
        begin = EDGE - count + 1 + tap
        conv = conv + taps_ref[tap : tap + 1] * padded[begin : begin + rows]
    gated = cbuf[:, 2 * channels :].astype(jnp.float32) * conv
    cvout[...] = (gated * group_scale(gated, GROUP) * cgain_ref[...]).astype(jnp.bfloat16)
    load_wo.wait()

    def partial(target):
        return jnp.dot(cvout[block_at(target), :], wobuf[...], preferred_element_type=jnp.float32)

    cross_copy = remote(cross, cross_in, cross_send, cross_recv, {"tp": near})
    fin_copy = remote(fin, fin_in, fin_send, fin_recv, {"tp": near})
    far_sum = remote(far, far_in, fs_send, fs_recv, {"tp": away})
    phase("partial")
    cross[...] = partial(diag).astype(jnp.bfloat16)
    cross_copy.start()
    fin[...] = partial(near).astype(jnp.bfloat16)
    fin_copy.start()
    out_ref[...] = partial(t)
    phase("relay_second")

    @pl.when(has_down & (is_top == 0))
    def _():
        relay(1, second, (1 - side,))

    def settle():
        toward = partial(away)
        cross_copy.wait_recv()
        far[...] = (toward + cross_in[...].astype(jnp.float32)).astype(jnp.bfloat16)
        far_sum.start()

    @pl.when(jnp.logical_not(relays))
    def _():
        settle()

    phase("q_late")
    prepare(1, second)
    phase("near1")

    @pl.when(job_level > 0)
    def _():
        @pl.when(jnp.logical_not(relays))
        def _():
            absorb(1, first, (0,), True)

        absorb(1, first, (1,), False)

    phase("toward")

    @pl.when(relays)
    def _():
        settle()

    phase("w_far")
    w_spread(1)
    @pl.when(has_down & (is_top * odd == 1))
    def _():
        relay(1, second, (1 - side,))

    @pl.when((level > 1) & relays)
    def _():
        relay(2, second, (side,))

    phase("near_loop")

    @pl.loop(2, job_level + 1)
    def _(j):
        @pl.when((j < level) & relays)
        def _():
            relay(j + 1, first)

        @pl.when((j > 2) | jnp.logical_not(relays))
        def _():
            absorb(j, first, (0,), True)

        absorb(j, first, (1,), False)

    @pl.when((level > 1) & relays)
    def _():
        relay(2, second, (1 - side,))

    phase("diag")
    diag_ready(1)
    run_tiles(
        diag_work([(1, 0, 1, 0), (1, 1, 1, 0), (1, 1, 1, 1), (1, 1, 0, 0), (0, 1, 1, 0)])
    )

    @pl.when(first == 1)
    def _():
        run_tiles(diag_work([(0, 0, 1, 0), (0, 1, 1, 1)]))

    @pl.when(first == 0)
    def _():
        run_tiles(diag_work([(1, 0, 0, 0), (1, 1, 0, 1)]))

    me8 = job_tp * 2 + side

    def piece_rows(which, target):
        return pl.ds(pl.multiple_of(which * rows + target * own, own), own)

    def o_copy(which, target, index):
        return remote(
            obuf.at[piece_rows(which, target)], hin.at[me8], o_send.at[index], o_recv.at[me8],
            {"sp": job_level * 2 + which, "tp": target},
        )

    def o_wait(which, source_tp, index):
        spot = hin.at[source_tp * 2 + which]
        return remote(spot, spot, o_send.at[index], o_recv.at[source_tp * 2 + which], mate_id)

    peers = [(1 - side, diag), (1 - side, away), (side, diag), (side, away)]
    peers += [(1 - side, t), (1 - side, near), (side, near)]

    def conclude(ph):
        span = slice(ph * rows, (ph + 1) * rows)
        other = slice(queries + ph * rows, queries + (ph + 1) * rows)
        for h in range(per):
            factor = lamb[swapped, side * per + h][0:1, 0:1]
            attn = acc[h, :, span] * (1.0 / total[h : h + 1, span])
            attn = attn - factor * (acc[h, :, other] * (1.0 / total[h : h + 1, other]))
            scale = lax.rsqrt(jnp.mean(attn * attn, axis=0, keepdims=True) + eps)
            result = ((attn * scale).T * sub_ref[...]).astype(jnp.bfloat16)
            cols = slice(h * vsize, (h + 1) * vsize)
            for which in range(2):
                base = which * half
                if ph == 0:
                    obuf[q_rows(which, first), cols] = result[base : base + half]
                else:
                    for part in range(2):
                        for b in range(2):
                            begin = which * rows + second * half + b * own + part * sub
                            at = base + part * own + b * sub
                            obuf[pl.ds(pl.multiple_of(begin, sub), sub), cols] = result[
                                at : at + sub
                            ]

    def store_logs():
        for h in range(per):
            logs = top[h : h + 1] + jnp.log(total[h : h + 1])
            for m in range(2):
                ordered = []
                for which in range(2):
                    at = m * queries + which * half
                    early_part = logs[:, at : at + half]
                    late_part = jnp.concatenate(
                        [
                            logs[:, at + rows + part * own + b * sub :][:, :sub]
                            for b in range(2)
                            for part in range(2)
                        ],
                        axis=1,
                    )
                    ordered.append(
                        jnp.concatenate(
                            [
                                jnp.where(first == 0, early_part, late_part),
                                jnp.where(first == 0, late_part, early_part),
                            ],
                            axis=1,
                        )
                    )
                low, high = ordered
                lout[0, h, m : m + 1, :] = jnp.where(side == 0, low, high)
                lout[1, h, m : m + 1, :] = jnp.where(side == 0, high, low)

    phase("far_loop")

    @pl.loop(1, job_level + 1)
    def _(j):
        absorb(j, second, (1,), True)

        @pl.when((j > 1) & (j < level) & relays)
        def _():
            relay(j + 1, second)

    phase("finish1")
    lam_copy.wait_recv()
    conclude(1)
    for index in range(4):
        which, target = peers[index]
        o_copy(which, target, index).start()
    phase("far_loop0")

    @pl.loop(1, job_level + 1)
    def _(j):
        absorb(j, second, (0,), False)

    phase("w_side")
    for c in range(W_PARTS):
        w_side(c).wait_recv()
        w_pass(1 - side, 1, c).start()

    def log_copy(index):
        which = side + index - 2 * index * side
        return remote(
            lout.at[index], lin.at[index], log_send.at[index], log_recv.at[index],
            {"sp": job_level * 2 + which, "tp": job_tp},
        )

    phase("finish0")
    conclude(0)
    for index in range(4, 7):
        which, target = peers[index]
        o_copy(which, target, index).start()

    @pl.when(swaps)
    def _():
        o_copy(side, t, 7).start()

    store_logs()
    log_copy(1).start()

    @pl.when(swaps)
    def _():
        log_copy(0).start()

    @pl.when(jnp.logical_not(swaps))
    def _():
        hin[me8] = obuf[piece_rows(side, t)]
        for h in range(per):
            log_ref[side * per + h] = lout[0, h]

    phase("conv_sum")
    fin_copy.wait_recv()
    far_sum.wait_recv()
    out_ref[...] += fin_in[...].astype(jnp.float32) + far_in[...].astype(jnp.float32)
    phase("w_wait")
    load_wa.wait()
    w_near.wait_recv()
    for c in range(W_PARTS):
        w_pass(side, 0, c).wait_recv()
        w_pass(1 - side, 1, c).wait_recv()
    phase("o_wait")
    for index, (which, source) in enumerate(peers):
        o_wait(which, source, index).wait_recv()

    @pl.when(swaps)
    def _():
        o_wait(side, t, 7).wait_recv()
        log_copy(0).wait_recv()
        for h in range(per):
            log_ref[side * per + h] = lin[0, h]

    phase("log")
    log_copy(1).wait_recv()
    for h in range(per):
        log_ref[(1 - side) * per + h] = lin[1, h]
    log_store = pltpu.make_async_copy(log_ref, log_hbm, out_sem.at[CHUNKS])
    log_store.start()

    phase("last_dot")
    lhs = jnp.concatenate([hin[i] for i in range(2 * tp)], axis=1)
    strip = out_ref.shape[1] // CHUNKS
    stores = [log_store]
    for c in range(CHUNKS):
        cols = slice(c * strip, (c + 1) * strip)
        out_ref[:, cols] += jnp.dot(lhs, wfull[:, cols], preferred_element_type=jnp.float32)
        store = pltpu.make_async_copy(out_ref.at[:, cols], out_hbm.at[:, cols], out_sem.at[c])
        store.start()
        stores.append(store)
    phase("sends")
    for store in stores:
        store.wait()
    near_copy.wait_send()
    for copy in far_copies + forwards:
        copy.wait_send()
    for pair, part in ((first, None), (second, 0), (second, 1)):
        give_copy(pair, part).wait_send()
        giveq_copy(pair, part).wait_send()
    w_near.wait_send()
    for c in range(W_PARTS):
        for copy in (w_far(c), w_side(c), w_pass(side, 0, c), w_pass(1 - side, 1, c)):
            copy.wait_send()
    for copy in (cross_copy, fin_copy, far_sum, log_copy(1), lam_copy):
        copy.wait_send()
    for index, (which, target) in enumerate(peers):
        o_copy(which, target, index).wait_send()

    @pl.when(swaps)
    def _():
        o_copy(side, t, 7).wait_send()
        log_copy(0).wait_send()
        for which in range(2):
            for pair in range(2):
                swap_q(which, pair).wait_send()

    @pl.loop(is_top * (1 - odd) * level, level + 1 - is_top * odd)
    def _(lev):
        for pair in range(2):
            for which in range(2):
                up_copy(lev, pair, which).wait_send()

    @pl.when(s < sp - 1)
    def _():
        tail_copy.wait_send()

    phase(None)


def phase(name):
    pass


def vmem():
    return pl.BlockSpec(memory_space=pltpu.VMEM)


def on_device(
    inputs, norm_gain, w_query, w_key, w_value, query_gain, key_gain, lambdas, sub_gain,
    w_gate_b, w_gate_c, w_conv_in, conv_taps, conv_gain, w_out_att, w_out_conv,
):
    heads = lambdas.shape[0]
    comp = query_gain.shape[1]
    vsize = sub_gain.shape[0]
    channels = conv_gain.shape[0]
    own, width = inputs.shape
    tp = lax.axis_size("tp")
    sp = lax.axis_size("sp")
    rows = own * tp
    half = rows // 2
    qcols = heads * 2 * comp
    mine = qcols // 2
    per = heads // 2
    dma = pltpu.SemaphoreType.DMA
    bf, f32 = jnp.bfloat16, jnp.float32
    weights = (w_key, w_value, w_query, w_gate_c, w_conv_in, w_gate_b, w_out_att, w_out_conv)
    groups = sp // 2 * 4
    piece = pltpu.VMEM((own, width), bf)
    any_spec = pl.BlockSpec(memory_space=pl.ANY)
    mixed, log_sums = pl.pallas_call(
        functools.partial(layer, sp, tp, comp, heads),
        out_shape=(
            jax.ShapeDtypeStruct((own, width), f32),
            jax.ShapeDtypeStruct((heads, 2, rows), f32),
        ),
        in_specs=[vmem()] * 4 + [pl.BlockSpec(memory_space=pltpu.SMEM)] + [vmem()] * 3
        + [any_spec] * 8,
        out_specs=(any_spec, any_spec),
        scratch_shapes=[
            pltpu.VMEM((own, width), f32),
            pltpu.VMEM((heads, 2, rows), f32),
            pltpu.VMEM((rows, width), bf),
            pltpu.VMEM((6, width, qcols), bf),
            pltpu.VMEM((tp * w_out_att.shape[0], width), bf),
            pltpu.VMEM(w_out_conv.shape, bf),
            pltpu.VMEM((8, qcols), f32),
            pltpu.VMEM((2, sp, 2 * half, 2 * mine), bf),
            pltpu.VMEM((3, per, vsize, 2 * half), bf),
            pltpu.VMEM((2, 2 * rows, mine), bf),
            pltpu.VMEM((2, half, 2 * mine), bf),
            pltpu.VMEM((2, half, mine), bf),
            pltpu.VMEM((per, 4 * rows, 2 * comp), bf),
            pltpu.VMEM((per, 4 * rows), f32),
            pltpu.VMEM((per, 4 * rows), f32),
            pltpu.VMEM((per, vsize, 4 * rows), f32),
            pltpu.VMEM((rows, 3 * channels), bf),
            pltpu.VMEM((EDGE, 2 * channels), bf),
            pltpu.VMEM((EDGE + rows, channels), f32),
            pltpu.VMEM((rows, channels), bf),
            pltpu.VMEM((2, heads, 8, 128), f32),
            piece, piece, piece, piece, piece, piece,
            pltpu.VMEM((2 * rows, per * vsize), bf),
            pltpu.VMEM((2 * tp, own, per * vsize), bf),
            pltpu.VMEM((2, per, 2, rows), f32),
            pltpu.VMEM((2, per, 2, rows), f32),
            dma((8,)), dma((2,)), dma((CHUNKS,)), dma((CHUNKS,)), dma((CHUNKS,)), dma((CHUNKS,)),
            dma((groups,)), dma((2 * groups,)), dma((3,)), dma((3,)), dma((3,)), dma((2,)),
            dma((2,)),
            dma((9,)), dma((9,)), dma(()), dma(()), dma(()), dma(()), dma(()), dma(()),
            dma((CHUNKS + 1,)), dma((8,)), dma((2 * tp,)), dma((2,)), dma((2,)), dma((2,)),
            dma((4,)), dma((4,)),
        ],
        compiler_params=pltpu.CompilerParams(
            collective_id=0, has_side_effects=True, vmem_limit_bytes=VMEM_LIMIT
        ),
        name="layer",
    )(
        inputs, norm_gain[None], query_gain, key_gain, lambdas, sub_gain[None], conv_taps,
        conv_gain[None], *weights,
    )
    return (mixed, log_sums)


def solution(mesh):
    in_specs = (
        P(("sp", "tp"), None),
        P(),
        P(None, "tp"),
        P(None, "tp"),
        P(None, "tp"),
        P(),
        P(),
        P("tp"),
        P(),
        P(None, "tp"),
        P(None, "tp"),
        P(None, "tp"),
        P(None, "tp"),
        P("tp"),
        P("tp", None),
        P("tp", None),
    )
    out_specs = (P(("sp", "tp"), None), P("tp", None, "sp"))
    return jax.shard_map(
        on_device, mesh=mesh, in_specs=in_specs, out_specs=out_specs, check_vma=False
    )
```

```python
import functools

import jax
import jax.numpy as jnp
from jax import lax
from jax.experimental import pallas as pl
from jax.experimental.pallas import tpu as pltpu
from jax.sharding import PartitionSpec as P

GROUP = 64
eps = 1e-06
MESH = pl.DeviceIdType.MESH
VMEM_LIMIT = 62 * 1024 * 1024
CHUNKS = 4
EDGE = 16
TILE = 128
DEPTH = 2
W_PARTS = 2


def rms_scale(values):
    return values * lax.rsqrt(jnp.mean(values * values, axis=-1, keepdims=True) + eps)


def flip(index, bit):
    return index + bit - 2 * bit * lax.rem(index // bit, 2)


def remote(src, dst, send, recv, where):
    return pltpu.make_async_remote_copy(
        src_ref=src, dst_ref=dst, send_sem=send, recv_sem=recv, device_id=where,
        device_id_type=MESH,
    )


def group_scale(values, size):
    lanes = values.shape[1]
    row = lax.broadcasted_iota(jnp.int32, (lanes, lanes), 0) // size
    col = lax.broadcasted_iota(jnp.int32, (lanes, lanes), 1) // size
    ones = jnp.where(row == col, 1.0, 0.0).astype(jnp.bfloat16)
    squares = values * values
    high = squares.astype(jnp.bfloat16)
    low = (squares - high.astype(jnp.float32)).astype(jnp.bfloat16)
    sums = jnp.dot(high, ones, preferred_element_type=jnp.float32) + jnp.dot(
        low, ones, preferred_element_type=jnp.float32
    )
    return lax.rsqrt(sums * (1.0 / size) + eps)


def layer(
    sp, tp, comp, heads,
    x_in, gain_in, qg_in, kg_in, lam_in, sub_in, taps_in, cgain_in,
    wk, wv, wq, wc, wi, wb, wa, wo,
    out_hbm, log_hbm, x_ref, gain_ref, qg_ref, kg_ref, lam_ref, sub_ref, taps_ref, cgain_ref,
    in_sem, out_ref, log_ref,
    held, wbuf, wfull, wobuf, gains, kvb, vt, qb, give_kv, give_q, qpad, top, total, acc, cbuf, tail,
    padded, cvout, lamb, cross, fin, far, cross_in, fin_in, far_in, obuf, hin, lout, lin,
    wsem, near_sem, far_send, far_recv, fwd_send, fwd_recv, up_send, kv_recv, gk_send, gq_send,
    q_recv, x_recv, tail_sem, w_send, w_recv, cross_send, cross_recv, fin_send, fin_recv, fs_send, fs_recv,
    out_sem, o_send, o_recv, log_send, log_recv, lam_sem, qs_send, qs_recv,
):
    s = lax.axis_index("sp")
    t = lax.axis_index("tp")
    level, side = s // 2, lax.rem(s, 2)
    levels = sp // 2
    mate = level * 2 + 1 - side
    near, away = flip(t, 1), flip(t, 2)
    diag = flip(near, 2)
    first, second = t // 2, 1 - t // 2
    own = x_ref.shape[0]
    rows = own * tp
    half = rows // 2
    head_cols = heads * 2 * comp // 2
    per = heads // 2
    vsize = sub_ref.shape[1]
    both = 2 * comp
    channels = cgain_ref.shape[1]
    has_up, has_down = level < levels - 1, level > 0

    def as_int(flag):
        return flag.astype(jnp.int32)

    ups, downs = as_int(has_up), as_int(has_down)
    mate_id = {"sp": mate}
    odd = lax.rem(t, 2)
    is_top, is_low = as_int(level == levels - 1), as_int(level == levels - 2)
    high_pair = is_top + is_low
    swapped = is_low * odd + is_top * (1 - odd)
    swaps = swapped == 1
    aside = is_low * (1 - odd) + is_top
    job_level = level + is_low * odd - is_top * (1 - odd)
    job_tp = t + swapped * (near - t)
    cross_sp = s + 2 * is_low - 2 * is_top
    cross_id = {"sp": cross_sp, "tp": near}
    up_id = {
        "sp": s + (1 - is_top) * (2 - 2 * is_low * (1 - odd)) - 2 * is_top * (1 - odd),
        "tp": t + aside * (near - t),
    }
    sends_own = is_top * odd == 0
    relays = is_top * (1 - odd) == 0
    groups = sp // 2 * 4

    small = (
        (x_in, x_ref), (gain_in, gain_ref), (kg_in, kg_ref), (qg_in, qg_ref), (lam_in, lam_ref),
        (sub_in, sub_ref), (taps_in, taps_ref), (cgain_in, cgain_ref),
    )
    reads = [
        pltpu.make_async_copy(src, dst, in_sem.at[i]) for i, (src, dst) in enumerate(small)
    ]
    for read in reads:
        read.start()
    loads = [
        pltpu.make_async_copy(w, wbuf.at[i], wsem.at[i])
        for i, w in enumerate((wk, wv, wq, wc, wi, wb))
    ]
    wa_rows = wa.shape[0]
    half_rows = wa_rows // 2

    def shard(index):
        return pl.ds(pl.multiple_of(index * wa_rows, wa_rows), wa_rows)

    w_part = half_rows // W_PARTS

    def part_of(index, which, c):
        begin = index * wa_rows + which * half_rows + c * w_part
        return pl.ds(pl.multiple_of(begin, w_part), w_part)

    load_wa = pltpu.make_async_copy(wa, wfull.at[shard(t)], wsem.at[6])
    load_wo = pltpu.make_async_copy(wo, wobuf, wsem.at[7])

    def block_at(index):
        return pl.ds(pl.multiple_of(index * own, own), own)

    phase("barrier")
    barrier = pltpu.get_barrier_semaphore()

    def hello(where):
        pl.semaphore_signal(barrier, inc=1, device_id=where, device_id_type=MESH)

    for peer in (near, away, diag):
        hello({"tp": peer})
    for peer in (t, near, away, diag):
        hello({"sp": mate, "tp": peer})

    plain_up = level < levels - 2
    plain_down = has_down & (level < levels - 1)

    @pl.when(plain_up)
    def _():
        hello({"sp": s + 2})

    @pl.when(plain_down)
    def _():
        hello({"sp": s - 2})

    @pl.when(high_pair == 1)
    def _():
        for which in range(2):
            for peer in range(tp):
                hello({"sp": (cross_sp // 2) * 2 + which, "tp": peer})

    @pl.when((side == 1) & has_up)
    def _():
        hello({"sp": s + 1})

    @pl.when((side == 0) & has_down)
    def _():
        hello({"sp": s - 1})

    phase("norm")
    for read in reads:
        read.wait()
    for load in (*loads, load_wa, load_wo):
        load.start()
    x = x_ref[...].astype(jnp.float32)
    held[block_at(t), :] = (rms_scale(x) * gain_ref[...]).astype(jnp.bfloat16)
    for row, ref in ((0, kg_ref), (1, qg_ref)):
        for h in range(heads):
            for m in range(2):
                at = (h * 2 + m) * comp
                gains[row : row + 1, at : at + comp] = ref[m : m + 1, :]

    phase("barrier_wait")
    expected = 7 + as_int(plain_up) + as_int(plain_down) + 2 * tp * high_pair
    pl.semaphore_wait(barrier, expected + side * ups + (1 - side) * downs)

    phase("defs")
    part = own // CHUNKS

    def chunk_at(index, c):
        return pl.ds(pl.multiple_of(index * own + c * part, part), part)

    def far_copy(c):
        spot = held.at[chunk_at(t, c)]
        return remote(spot, spot, far_send.at[c], far_recv.at[c], {"tp": away})

    def forward(c):
        spot = held.at[chunk_at(away, c)]
        return remote(spot, spot, fwd_send.at[c], fwd_recv.at[c], {"tp": near})

    far_copies = [far_copy(c) for c in range(CHUNKS)]
    forwards = [forward(c) for c in range(CHUNKS)]
    mine = held.at[block_at(t)]
    near_copy = remote(mine, mine, near_sem.at[0], near_sem.at[1], {"tp": near})
    near_copy.start()
    for copy in far_copies:
        copy.start()
    for h in range(heads):
        lamb[0, h] = jnp.full(lamb.shape[2:], lam_ref[h], jnp.float32)
    lam_copy = remote(lamb.at[0], lamb.at[1], lam_sem.at[0], lam_sem.at[1], {"tp": near})
    lam_copy.start()

    w_near = remote(wa, wfull.at[shard(t)], w_send.at[0], w_recv.at[0], {"tp": near})
    def w_far(c):
        return remote(
            wa.at[pl.ds(pl.multiple_of(side * half_rows + c * w_part, w_part), w_part)],
            wfull.at[part_of(t, side, c)], w_send.at[1 + c], w_recv.at[1 + c], {"tp": away},
        )

    def w_side(c):
        spot = wfull.at[part_of(away, side, c)]
        return remote(spot, spot, w_send.at[3 + c], w_recv.at[3 + c], mate_id)

    def w_pass(which, kind, c):
        spot = wfull.at[part_of(away, which, c)]
        slot = 5 + 2 * kind + c
        return remote(spot, spot, w_send.at[slot], w_recv.at[slot], {"tp": near})

    def w_spread(c):
        w_far(c).wait_recv()
        w_side(c).start()
        w_pass(side, 0, c).start()

    def slot_of(lev, pair):
        return lev * 2 + pair

    def group_of(lev, pair, which):
        return (lev * 2 + pair) * 2 + which

    def side_rows(which):
        return pl.ds(pl.multiple_of(which * half, half), half)

    def up_copy(lev, pair, which):
        g = group_of(lev, pair, which)
        return remote(
            kvb.at[0, slot_of(lev, pair), side_rows(which)],
            kvb.at[aside, slot_of(lev, pair), side_rows(which)],
            up_send.at[g], kv_recv.at[aside * groups + g], up_id,
        )

    def arrived(where, lev, pair, which):
        spot = kvb.at[where, slot_of(lev, pair), side_rows(which)]
        g = group_of(lev, pair, which)
        remote(spot, spot, up_send.at[g], kv_recv.at[where * groups + g], up_id).wait_recv()

    sub = own // 2

    def part_span(base, part):
        if part is None:
            return pl.ds(pl.multiple_of(base, half), half)
        return pl.ds(pl.multiple_of(base + part * own, own), own)

    def give_copy(pair, part):
        index = 0 if part is None else 1 + part
        arrival = kv_recv.at[group_of(level, pair, side)] if part is None else x_recv.at[part]
        return remote(
            give_kv.at[pair, part_span(0, part)],
            kvb.at[0, slot_of(level, pair), part_span(side * half, part)],
            gk_send.at[index], arrival, mate_id,
        )

    def q_rows(which, pair):
        return pl.ds(pl.multiple_of(which * rows + pair * half, half), half)

    def giveq_copy(pair, part):
        index = 0 if part is None else 1 + part
        return remote(
            give_q.at[pair, part_span(0, part)],
            qb.at[0, part_span(side * rows + pair * half, part)],
            gq_send.at[index], q_recv.at[index], mate_id,
        )

    def swap_q(which, pair):
        index = which * 2 + pair
        return remote(
            qb.at[0, q_rows(which, pair)], qb.at[1, q_rows(which, pair)],
            qs_send.at[index], qs_recv.at[index], cross_id,
        )

    def pass_q(which, pair):
        @pl.when(swaps)
        def _():
            swap_q(which, pair).start()

    def split(values):
        low, high = values[:, :head_cols], values[:, head_cols:]
        return jnp.where(side == 0, low, high), jnp.where(side == 0, high, low)

    def pair_rows(pair):
        return pl.ds(pl.multiple_of(pair * half, half), half)

    def scaled(block, i, gain_row, factor):
        res = jnp.dot(block, wbuf[i], preferred_element_type=jnp.float32).astype(jnp.bfloat16)
        wide = res.astype(jnp.float32)
        return (wide * group_scale(wide, comp) * (gains[gain_row : gain_row + 1] * factor)).astype(
            jnp.bfloat16
        )

    def source(pair, part):
        if part is None:
            return held[pair_rows(pair)]
        return jnp.concatenate(
            [
                held[pl.ds(pl.multiple_of(pair * half + b * own + part * sub, sub), sub)]
                for b in range(2)
            ],
            axis=0,
        )

    def project_kv(pair, part=None):
        block = source(pair, part)
        slot = slot_of(level, pair)
        for i in range(2):
            if i == 0:
                res = scaled(block, 0, 0, 1.0)
            else:
                res = jnp.dot(block, wbuf[1], preferred_element_type=jnp.float32).astype(
                    jnp.bfloat16
                )
            keep, give = split(res)
            cols = slice(i * head_cols, (i + 1) * head_cols)
            kvb[0, slot, part_span(side * half, part), cols] = keep
            give_kv[pair, part_span(0, part), cols] = give

        give_copy(pair, part).start()
        if part != 0:
            @pl.when(sends_own)
            def _():
                up_copy(level, pair, side).start()

    def project_q(pair, part=None):
        block = source(pair, part)
        keep, give = split(scaled(block, 2, 1, comp ** (-0.5)))
        qb[0, part_span(side * rows + pair * half, part)] = keep
        give_q[pair, part_span(0, part)] = give
        giveq_copy(pair, part).start()
        if part != 0:
            pass_q(side, pair)

    def project_conv(pair, part=None):
        block = source(pair, part)
        for i in range(3):
            res = jnp.dot(block, wbuf[3 + i], preferred_element_type=jnp.float32).astype(
                jnp.bfloat16
            )
            cols = slice(i * channels, (i + 1) * channels)
            if part is None:
                cbuf[pair_rows(pair), cols] = res
            else:
                for b in range(2):
                    begin = pl.multiple_of(pair * half + b * own + part * sub, sub)
                    cbuf[pl.ds(begin, sub), cols] = res[b * sub : (b + 1) * sub]

    def await_mate(pair, parts):
        if parts is None:
            arrived(0, level, pair, 1 - side)
        else:
            for part in parts:
                give_copy(pair, part).wait_recv()

        @pl.when(sends_own)
        def _():
            up_copy(level, pair, 1 - side).start()

    def relay(j, pair, sides=(side, 1 - side)):
        for which in sides:
            arrived(0, level - j, pair, which)
            up_copy(level - j, pair, which).start()

    queries = 2 * rows
    tile = min(TILE, half)

    def prepare(phase_index, pair):
        for which in range(2):
            @pl.when(swaps)
            def _():
                swap_q(which, pair).wait_recv()

            lane = lax.broadcasted_iota(jnp.int32, (half, both), 1)
            for h in range(per):
                q = qb[swapped, q_rows(which, pair), h * both : (h + 1) * both]
                zero = jnp.zeros_like(q)
                at = phase_index * rows + which * half
                qpad[h, at : at + half] = jnp.where(lane < comp, q, zero)
                qpad[h, queries + at : queries + at + half] = jnp.where(lane < comp, zero, q)

    def position(index):
        low = index % own
        return low // sub * own + index // own * sub + low % sub

    def run_tiles(work):
        def score(item):
            h, keys, values, at, mask = item
            return lax.dot_general(
                keys(), qpad[h, at], (((1,), (1,)), ((), ())), preferred_element_type=jnp.float32
            )

        def finish(item):
            h, values, at, p, factor = item
            acc[h, :, at] = acc[h, :, at] * factor + jnp.dot(
                values(), p, preferred_element_type=jnp.float32
            )

        ahead = [score(item) for item in work[:DEPTH]]
        late = None
        for index, (h, keys, values, at, mask) in enumerate(work):
            scores = ahead.pop(0)
            if index + DEPTH < len(work):
                ahead.append(score(work[index + DEPTH]))
            if mask is not None:
                kpos = lax.broadcasted_iota(jnp.int32, scores.shape, 0)
                qpos = mask[0] + lax.broadcasted_iota(jnp.int32, scores.shape, 1)
                if mask[1]:
                    kpos, qpos = position(kpos), position(qpos)
                scores = jnp.where(kpos <= qpos, scores, -1e30)
            old = top[h : h + 1, at]
            new = jnp.maximum(old, jnp.max(scores, axis=0, keepdims=True))
            p = jnp.exp(scores - new)
            factor = jnp.exp(old - new)
            top[h : h + 1, at] = new
            total[h : h + 1, at] = total[h : h + 1, at] * factor + jnp.sum(
                p, axis=0, keepdims=True
            )
            if late is not None:
                finish(late)
            late = (h, values, at, p.astype(jnp.bfloat16), factor)
        finish(late)

    def key_part(slot, h, begin, size):
        return lambda: kvb[swapped, slot, begin : begin + size, h * both : (h + 1) * both]

    def value_part(where, h, begin, size):
        return lambda: vt[where, h, :, begin : begin + size]

    def turn_values(slot, where):
        for h in range(per):
            cols = slice(head_cols + h * vsize, head_cols + (h + 1) * vsize)
            vt[where, h] = kvb[swapped, slot, :, cols].T

    def taken(lev, pair):
        @pl.when(swaps)
        def _():
            for which in range(2):
                arrived(1, lev, pair, which)

    def absorb(j, pair, phases, take):
        lev = job_level - j
        if take:
            taken(lev, pair)
        slot = slot_of(lev, pair)
        turn_values(slot, 0)
        run_tiles(
            [
                (
                    h, key_part(slot, h, which * half, half),
                    value_part(0, h, which * half, half), slice(start, start + tile), None,
                )
                for h in range(per)
                for ph in phases
                for m in range(2)
                for start in range(
                    m * queries + ph * rows, m * queries + (ph + 1) * rows, tile
                )
                for which in range(2)
            ]
        )

    pairs = (first, second)

    def diag_work(blocks):
        work = []
        for h in range(per):
            for q_ph, q_side, k_ph, k_side in blocks:
                same = q_ph == k_ph and q_side == k_side
                slot = slot_of(job_level, pairs[k_ph])
                for m in range(2):
                    base = m * queries + q_ph * rows + q_side * half
                    for offset in range(0, half, tile):
                        size = offset + tile if same and q_ph == 0 else half
                        work.append(
                            (
                                h, key_part(slot, h, k_side * half, size),
                                value_part(1 + k_ph, h, k_side * half, size),
                                slice(base + offset, base + offset + tile),
                                (offset, q_ph == 1) if same else None,
                            )
                        )
        return work

    def diag_ready(ph):
        taken(job_level, pairs[ph])
        turn_values(slot_of(job_level, pairs[ph]), 1 + ph)

    phase("wait_kv_weights")
    loads[0].wait()
    loads[1].wait()
    phase("wait_near")
    near_copy.wait_recv()
    phase("kv_first")
    project_kv(first)
    w_near.start()
    phase("q_first")
    loads[2].wait()
    project_q(first)
    phase("conv_first")
    for load in loads[3:]:
        load.wait()
    project_conv(first)
    tail_copy = remote(
        cbuf.at[pl.ds(rows - EDGE, EDGE), pl.ds(0, 2 * channels)], tail,
        tail_sem.at[0], tail_sem.at[1], {"sp": jnp.minimum(s + 1, sp - 1)},
    )

    @pl.when((s < sp - 1) & (first == 1))
    def _():
        tail_copy.start()

    phase("mate_first")
    await_mate(first, None)
    phase("part_a")
    for c in range(CHUNKS // 2):
        far_copies[c].wait_recv()
        forwards[c].start()
    for c in range(CHUNKS // 2):
        forwards[c].wait_recv()
    project_kv(second, 0)
    project_q(second, 0)
    project_conv(second, 0)

    phase("below_first")
    @pl.when(has_down & relays)
    def _():
        relay(1, first)

    giveq_copy(first, None).wait_recv()
    pass_q(1 - side, first)
    phase("early")
    top[...] = jnp.full_like(top, -1e30)
    total[...] = jnp.zeros_like(total)
    acc[...] = jnp.zeros_like(acc)

    def early():
        prepare(0, first)
        diag_ready(0)
        run_tiles(diag_work([(0, 0, 0, 0), (0, 1, 0, 0), (0, 1, 0, 1)]))

    for c in range(CHUNKS // 2, CHUNKS - 1):
        far_copies[c].wait_recv()
        forwards[c].start()

    for c in range(W_PARTS):
        w_far(c).start()

    @pl.when(jnp.logical_not(swaps))
    def _():
        early()

    phase("far_wait")
    far_copies[CHUNKS - 1].wait_recv()
    forwards[CHUNKS - 1].start()
    for copy in forwards[CHUNKS // 2 :]:
        copy.wait_recv()
    phase("kv_second")
    project_kv(second, 1)
    phase("q_second")
    project_q(second, 1)
    phase("conv_second")
    project_conv(second, 1)

    @pl.when((s < sp - 1) & (first == 0))
    def _():
        tail_copy.start()

    phase("below_first2")

    @pl.when((level > 1) & relays)
    def _():
        relay(2, first)

    phase("early2a")

    @pl.when(swaps & relays)
    def _():
        early()

    @pl.when(jnp.logical_not(swaps) & (job_level > 0))
    def _():
        absorb(1, first, (0,), True)

    phase("mate_second")
    await_mate(second, (0, 1))

    @pl.when(swaps)
    def _():
        for part in range(2):
            giveq_copy(second, part).wait_recv()
        swap_q(1 - side, second).start()

    phase("early2")

    @pl.when(jnp.logical_not(relays))
    def _():
        early()

    @pl.when(relays)
    def _():
        @pl.loop(2 - swapped, jnp.minimum(job_level, 2) + 1)
        def _(j):
            absorb(j, first, (0,), True)

    @pl.when(jnp.logical_not(swaps))
    def _():
        for part in range(2):
            giveq_copy(second, part).wait_recv()

    @pl.when(has_down & relays)
    def _():
        relay(1, second, (side,))

    phase("w_first")
    w_spread(0)
    phase("conv")
    def product(ref):
        gate = ref[:, :channels].astype(jnp.float32)
        other = ref[:, channels : 2 * channels].astype(jnp.float32)
        return (gate * other).astype(jnp.bfloat16).astype(jnp.float32)

    padded[EDGE:] = product(cbuf)

    @pl.when(s > 0)
    def _():
        tail_copy.wait_recv()
        padded[:EDGE] = product(tail)

    @pl.when(s == 0)
    def _():
        padded[:EDGE] = jnp.zeros((EDGE, channels), jnp.float32)

    count = taps_ref.shape[0]
    conv = jnp.zeros((rows, channels), jnp.float32)
    for tap in range(count):
        begin = EDGE - count + 1 + tap
        conv = conv + taps_ref[tap : tap + 1] * padded[begin : begin + rows]
    gated = cbuf[:, 2 * channels :].astype(jnp.float32) * conv
    cvout[...] = (gated * group_scale(gated, GROUP) * cgain_ref[...]).astype(jnp.bfloat16)
    load_wo.wait()

    def partial(target):
        return jnp.dot(cvout[block_at(target), :], wobuf[...], preferred_element_type=jnp.float32)

    cross_copy = remote(cross, cross_in, cross_send, cross_recv, {"tp": near})
    fin_copy = remote(fin, fin_in, fin_send, fin_recv, {"tp": near})
    far_sum = remote(far, far_in, fs_send, fs_recv, {"tp": away})
    phase("partial")
    cross[...] = partial(diag).astype(jnp.bfloat16)
    cross_copy.start()
    fin[...] = partial(near).astype(jnp.bfloat16)
    fin_copy.start()
    out_ref[...] = partial(t)
    phase("relay_second")

    @pl.when(has_down & (is_top == 0))
    def _():
        relay(1, second, (1 - side,))

    def settle():
        toward = partial(away)
        cross_copy.wait_recv()
        far[...] = (toward + cross_in[...].astype(jnp.float32)).astype(jnp.bfloat16)
        far_sum.start()

    @pl.when(jnp.logical_not(relays))
    def _():
        settle()

    phase("q_late")
    prepare(1, second)
    phase("near1")

    @pl.when(job_level > 0)
    def _():
        @pl.when(jnp.logical_not(relays))
        def _():
            absorb(1, first, (0,), True)

        absorb(1, first, (1,), False)

    phase("toward")

    @pl.when(relays)
    def _():
        settle()

    phase("w_far")
    w_spread(1)
    @pl.when(has_down & (is_top * odd == 1))
    def _():
        relay(1, second, (1 - side,))

    phase("near_loop")

    @pl.loop(2, job_level + 1)
    def _(j):
        @pl.when((j < level) & relays)
        def _():
            relay(j + 1, first)

        @pl.when((j > 2) | jnp.logical_not(relays))
        def _():
            absorb(j, first, (0,), True)

        absorb(j, first, (1,), False)

        @pl.when((j == 2) & (level > 1) & relays)
        def _():
            relay(2, second, (side,))

    @pl.when((level > 1) & relays)
    def _():
        relay(2, second, (1 - side,))

    phase("diag")
    diag_ready(1)
    run_tiles(
        diag_work([(1, 0, 1, 0), (1, 1, 1, 0), (1, 1, 1, 1), (1, 1, 0, 0), (0, 1, 1, 0)])
    )

    @pl.when(first == 1)
    def _():
        run_tiles(diag_work([(0, 0, 1, 0), (0, 1, 1, 1)]))

    @pl.when(first == 0)
    def _():
        run_tiles(diag_work([(1, 0, 0, 0), (1, 1, 0, 1)]))

    me8 = job_tp * 2 + side

    def piece_rows(which, target):
        return pl.ds(pl.multiple_of(which * rows + target * own, own), own)

    def o_copy(which, target, index):
        return remote(
            obuf.at[piece_rows(which, target)], hin.at[me8], o_send.at[index], o_recv.at[me8],
            {"sp": job_level * 2 + which, "tp": target},
        )

    def o_wait(which, source_tp, index):
        spot = hin.at[source_tp * 2 + which]
        return remote(spot, spot, o_send.at[index], o_recv.at[source_tp * 2 + which], mate_id)

    peers = [(1 - side, diag), (1 - side, away), (side, diag), (side, away)]
    peers += [(1 - side, t), (1 - side, near), (side, near)]

    def conclude(ph):
        span = slice(ph * rows, (ph + 1) * rows)
        other = slice(queries + ph * rows, queries + (ph + 1) * rows)
        for h in range(per):
            factor = lamb[swapped, side * per + h][0:1, 0:1]
            attn = acc[h, :, span] * (1.0 / total[h : h + 1, span])
            attn = attn - factor * (acc[h, :, other] * (1.0 / total[h : h + 1, other]))
            scale = lax.rsqrt(jnp.mean(attn * attn, axis=0, keepdims=True) + eps)
            result = ((attn * scale).T * sub_ref[...]).astype(jnp.bfloat16)
            cols = slice(h * vsize, (h + 1) * vsize)
            for which in range(2):
                base = which * half
                if ph == 0:
                    obuf[q_rows(which, first), cols] = result[base : base + half]
                else:
                    for part in range(2):
                        for b in range(2):
                            begin = which * rows + second * half + b * own + part * sub
                            at = base + part * own + b * sub
                            obuf[pl.ds(pl.multiple_of(begin, sub), sub), cols] = result[
                                at : at + sub
                            ]

    def store_logs():
        for h in range(per):
            logs = top[h : h + 1] + jnp.log(total[h : h + 1])
            for m in range(2):
                ordered = []
                for which in range(2):
                    at = m * queries + which * half
                    early_part = logs[:, at : at + half]
                    late_part = jnp.concatenate(
                        [
                            logs[:, at + rows + part * own + b * sub :][:, :sub]
                            for b in range(2)
                            for part in range(2)
                        ],
                        axis=1,
                    )
                    ordered.append(
                        jnp.concatenate(
                            [
                                jnp.where(first == 0, early_part, late_part),
                                jnp.where(first == 0, late_part, early_part),
                            ],
                            axis=1,
                        )
                    )
                low, high = ordered
                lout[0, h, m : m + 1, :] = jnp.where(side == 0, low, high)
                lout[1, h, m : m + 1, :] = jnp.where(side == 0, high, low)

    phase("far_loop")

    @pl.loop(1, job_level + 1)
    def _(j):
        absorb(j, second, (1,), True)

        @pl.when((j > 1) & (j < level) & relays)
        def _():
            relay(j + 1, second)

    phase("finish1")
    lam_copy.wait_recv()
    conclude(1)
    for index in range(4):
        which, target = peers[index]
        o_copy(which, target, index).start()
    phase("far_loop0")

    @pl.loop(1, job_level + 1)
    def _(j):
        absorb(j, second, (0,), False)

    phase("w_side")
    for c in range(W_PARTS):
        w_side(c).wait_recv()
        w_pass(1 - side, 1, c).start()

    def log_copy(index):
        which = side + index - 2 * index * side
        return remote(
            lout.at[index], lin.at[index], log_send.at[index], log_recv.at[index],
            {"sp": job_level * 2 + which, "tp": job_tp},
        )

    phase("finish0")
    store_logs()
    log_copy(1).start()

    @pl.when(swaps)
    def _():
        log_copy(0).start()

    conclude(0)
    for index in range(4, 7):
        which, target = peers[index]
        o_copy(which, target, index).start()

    @pl.when(swaps)
    def _():
        o_copy(side, t, 7).start()

    @pl.when(jnp.logical_not(swaps))
    def _():
        hin[me8] = obuf[piece_rows(side, t)]
        for h in range(per):
            log_ref[side * per + h] = lout[0, h]

    phase("conv_sum")
    fin_copy.wait_recv()
    far_sum.wait_recv()
    out_ref[...] += fin_in[...].astype(jnp.float32) + far_in[...].astype(jnp.float32)
    phase("w_wait")
    load_wa.wait()
    w_near.wait_recv()
    for c in range(W_PARTS):
        w_pass(side, 0, c).wait_recv()
        w_pass(1 - side, 1, c).wait_recv()
    phase("o_wait")
    for index, (which, source) in enumerate(peers):
        o_wait(which, source, index).wait_recv()

    @pl.when(swaps)
    def _():
        o_wait(side, t, 7).wait_recv()
        log_copy(0).wait_recv()
        for h in range(per):
            log_ref[side * per + h] = lin[0, h]

    phase("last_dot")
    lhs = jnp.concatenate([hin[i] for i in range(2 * tp)], axis=1)
    strip = out_ref.shape[1] // CHUNKS
    stores = []
    for c in range(CHUNKS):
        cols = slice(c * strip, (c + 1) * strip)
        out_ref[:, cols] += jnp.dot(lhs, wfull[:, cols], preferred_element_type=jnp.float32)
        store = pltpu.make_async_copy(out_ref.at[:, cols], out_hbm.at[:, cols], out_sem.at[c])
        store.start()
        stores.append(store)
    phase("log")
    log_copy(1).wait_recv()
    for h in range(per):
        log_ref[(1 - side) * per + h] = lin[1, h]
    log_store = pltpu.make_async_copy(log_ref, log_hbm, out_sem.at[CHUNKS])
    log_store.start()
    stores.append(log_store)
    phase("sends")
    for store in stores:
        store.wait()
    near_copy.wait_send()
    for copy in far_copies + forwards:
        copy.wait_send()
    for pair, part in ((first, None), (second, 0), (second, 1)):
        give_copy(pair, part).wait_send()
        giveq_copy(pair, part).wait_send()
    w_near.wait_send()
    for c in range(W_PARTS):
        for copy in (w_far(c), w_side(c), w_pass(side, 0, c), w_pass(1 - side, 1, c)):
            copy.wait_send()
    for copy in (cross_copy, fin_copy, far_sum, log_copy(1), lam_copy):
        copy.wait_send()
    for index, (which, target) in enumerate(peers):
        o_copy(which, target, index).wait_send()

    @pl.when(swaps)
    def _():
        o_copy(side, t, 7).wait_send()
        log_copy(0).wait_send()
        for which in range(2):
            for pair in range(2):
                swap_q(which, pair).wait_send()

    @pl.loop(is_top * (1 - odd) * level, level + 1 - is_top * odd)
    def _(lev):
        for pair in range(2):
            for which in range(2):
                up_copy(lev, pair, which).wait_send()

    @pl.when(s < sp - 1)
    def _():
        tail_copy.wait_send()

    phase(None)


def phase(name):
    pass


def on_device(
    inputs, norm_gain, w_query, w_key, w_value, query_gain, key_gain, lambdas, sub_gain,
    w_gate_b, w_gate_c, w_conv_in, conv_taps, conv_gain, w_out_att, w_out_conv,
):
    heads = lambdas.shape[0]
    comp = query_gain.shape[1]
    vsize = sub_gain.shape[0]
    channels = conv_gain.shape[0]
    own, width = inputs.shape
    tp = lax.axis_size("tp")
    sp = lax.axis_size("sp")
    rows = own * tp
    half = rows // 2
    qcols = heads * 2 * comp
    mine = qcols // 2
    per = heads // 2
    dma = pltpu.SemaphoreType.DMA
    bf, f32 = jnp.bfloat16, jnp.float32
    weights = (w_key, w_value, w_query, w_gate_c, w_conv_in, w_gate_b, w_out_att, w_out_conv)
    groups = sp // 2 * 4
    piece = pltpu.VMEM((own, width), bf)
    any_spec = pl.BlockSpec(memory_space=pl.ANY)
    mixed, log_sums = pl.pallas_call(
        functools.partial(layer, sp, tp, comp, heads),
        out_shape=(
            jax.ShapeDtypeStruct((own, width), f32),
            jax.ShapeDtypeStruct((heads, 2, rows), f32),
        ),
        in_specs=[any_spec] * 16,
        out_specs=(any_spec, any_spec),
        scratch_shapes=[
            pltpu.VMEM(inputs.shape, inputs.dtype),
            pltpu.VMEM((1, width), f32),
            pltpu.VMEM(query_gain.shape, f32),
            pltpu.VMEM(key_gain.shape, f32),
            pltpu.SMEM(lambdas.shape, f32),
            pltpu.VMEM((1, vsize), f32),
            pltpu.VMEM(conv_taps.shape, f32),
            pltpu.VMEM((1, channels), f32),
            dma((8,)),
            pltpu.VMEM((own, width), f32),
            pltpu.VMEM((heads, 2, rows), f32),
            pltpu.VMEM((rows, width), bf),
            pltpu.VMEM((6, width, qcols), bf),
            pltpu.VMEM((tp * w_out_att.shape[0], width), bf),
            pltpu.VMEM(w_out_conv.shape, bf),
            pltpu.VMEM((8, qcols), f32),
            pltpu.VMEM((2, sp, 2 * half, 2 * mine), bf),
            pltpu.VMEM((3, per, vsize, 2 * half), bf),
            pltpu.VMEM((2, 2 * rows, mine), bf),
            pltpu.VMEM((2, half, 2 * mine), bf),
            pltpu.VMEM((2, half, mine), bf),
            pltpu.VMEM((per, 4 * rows, 2 * comp), bf),
            pltpu.VMEM((per, 4 * rows), f32),
            pltpu.VMEM((per, 4 * rows), f32),
            pltpu.VMEM((per, vsize, 4 * rows), f32),
            pltpu.VMEM((rows, 3 * channels), bf),
            pltpu.VMEM((EDGE, 2 * channels), bf),
            pltpu.VMEM((EDGE + rows, channels), f32),
            pltpu.VMEM((rows, channels), bf),
            pltpu.VMEM((2, heads, 8, 128), f32),
            piece, piece, piece, piece, piece, piece,
            pltpu.VMEM((2 * rows, per * vsize), bf),
            pltpu.VMEM((2 * tp, own, per * vsize), bf),
            pltpu.VMEM((2, per, 2, rows), f32),
            pltpu.VMEM((2, per, 2, rows), f32),
            dma((8,)), dma((2,)), dma((CHUNKS,)), dma((CHUNKS,)), dma((CHUNKS,)), dma((CHUNKS,)),
            dma((groups,)), dma((2 * groups,)), dma((3,)), dma((3,)), dma((3,)), dma((2,)),
            dma((2,)),
            dma((9,)), dma((9,)), dma(()), dma(()), dma(()), dma(()), dma(()), dma(()),
            dma((CHUNKS + 1,)), dma((8,)), dma((2 * tp,)), dma((2,)), dma((2,)), dma((2,)),
            dma((4,)), dma((4,)),
        ],
        compiler_params=pltpu.CompilerParams(
            collective_id=0, has_side_effects=True, vmem_limit_bytes=VMEM_LIMIT
        ),
        name="layer",
    )(
        inputs, norm_gain[None], query_gain, key_gain, lambdas, sub_gain[None], conv_taps,
        conv_gain[None], *weights,
    )
    return (mixed, log_sums)


def solution(mesh):
    in_specs = (
        P(("sp", "tp"), None),
        P(),
        P(None, "tp"),
        P(None, "tp"),
        P(None, "tp"),
        P(),
        P(),
        P("tp"),
        P(),
        P(None, "tp"),
        P(None, "tp"),
        P(None, "tp"),
        P(None, "tp"),
        P("tp"),
        P("tp", None),
        P("tp", None),
    )
    out_specs = (P(("sp", "tp"), None), P("tp", None, "sp"))
    return jax.shard_map(
        on_device, mesh=mesh, in_specs=in_specs, out_specs=out_specs, check_vma=False
    )
```

```python
import functools

import jax
import jax.numpy as jnp
from jax import lax
from jax.experimental import pallas as pl
from jax.experimental.pallas import tpu as pltpu
from jax.sharding import PartitionSpec as P

GROUP = 64
eps = 1e-06
MESH = pl.DeviceIdType.MESH
VMEM_LIMIT = 62 * 1024 * 1024
CHUNKS = 4
EDGE = 16
TILE = 128
DEPTH = 2
W_PARTS = 2


def rms_scale(values):
    return values * lax.rsqrt(jnp.mean(values * values, axis=-1, keepdims=True) + eps)


def flip(index, bit):
    return index + bit - 2 * bit * lax.rem(index // bit, 2)


def remote(src, dst, send, recv, where):
    return pltpu.make_async_remote_copy(
        src_ref=src, dst_ref=dst, send_sem=send, recv_sem=recv, device_id=where,
        device_id_type=MESH,
    )


def group_scale(values, size):
    lanes = values.shape[1]
    row = lax.broadcasted_iota(jnp.int32, (lanes, lanes), 0) // size
    col = lax.broadcasted_iota(jnp.int32, (lanes, lanes), 1) // size
    ones = jnp.where(row == col, 1.0, 0.0).astype(jnp.bfloat16)
    squares = values * values
    high = squares.astype(jnp.bfloat16)
    low = (squares - high.astype(jnp.float32)).astype(jnp.bfloat16)
    sums = jnp.dot(high, ones, preferred_element_type=jnp.float32) + jnp.dot(
        low, ones, preferred_element_type=jnp.float32
    )
    return lax.rsqrt(sums * (1.0 / size) + eps)


def layer(
    sp, tp, comp, heads,
    x_in, gain_in, qg_in, kg_in, lam_in, sub_in, taps_in, cgain_in,
    wk, wv, wq, wc, wi, wb, wa, wo,
    out_hbm, log_hbm, x_ref, gain_ref, qg_ref, kg_ref, lam_ref, sub_ref, taps_ref, cgain_ref,
    out_ref, log_ref,
    held, wbuf, wfull, wobuf, gains, kvb, vt, qb, give_kv, give_q, qpad, top, total, acc, cbuf, tail,
    padded, cvout, lamb, cross, fin, far, cross_in, fin_in, far_in, obuf, hin, lout, lin,
    wsem, near_sem, far_send, far_recv, fwd_send, fwd_recv, up_send, kv_recv, gk_send, gq_send,
    q_recv, x_recv, tail_sem, w_send, w_recv, cross_send, cross_recv, fin_send, fin_recv, fs_send, fs_recv,
    o_send, o_recv, log_send, log_recv, lam_sem, qs_send, qs_recv,
):
    s = lax.axis_index("sp")
    t = lax.axis_index("tp")
    level, side = s // 2, lax.rem(s, 2)
    levels = sp // 2
    mate = level * 2 + 1 - side
    near, away = flip(t, 1), flip(t, 2)
    diag = flip(near, 2)
    first, second = t // 2, 1 - t // 2
    own = x_ref.shape[0]
    rows = own * tp
    half = rows // 2
    head_cols = heads * 2 * comp // 2
    per = heads // 2
    vsize = sub_ref.shape[1]
    both = 2 * comp
    channels = cgain_ref.shape[1]
    has_up, has_down = level < levels - 1, level > 0

    def as_int(flag):
        return flag.astype(jnp.int32)

    ups, downs = as_int(has_up), as_int(has_down)
    mate_id = {"sp": mate}
    odd = lax.rem(t, 2)
    is_top, is_low = as_int(level == levels - 1), as_int(level == levels - 2)
    high_pair = is_top + is_low
    swapped = is_low * odd + is_top * (1 - odd)
    swaps = swapped == 1
    aside = is_low * (1 - odd) + is_top
    job_level = level + is_low * odd - is_top * (1 - odd)
    job_tp = t + swapped * (near - t)
    cross_sp = s + 2 * is_low - 2 * is_top
    cross_id = {"sp": cross_sp, "tp": near}
    up_id = {
        "sp": s + (1 - is_top) * (2 - 2 * is_low * (1 - odd)) - 2 * is_top * (1 - odd),
        "tp": t + aside * (near - t),
    }
    sends_own = is_top * odd == 0
    relays = is_top * (1 - odd) == 0
    groups = sp // 2 * 4

    small = (
        (x_in, x_ref), (gain_in, gain_ref), (kg_in, kg_ref), (qg_in, qg_ref), (lam_in, lam_ref),
        (sub_in, sub_ref), (taps_in, taps_ref), (cgain_in, cgain_ref),
    )
    reads = [
        pltpu.make_async_copy(src, dst, wsem.at[i]) for i, (src, dst) in enumerate(small)
    ]
    for read in reads:
        read.start()
    loads = [
        pltpu.make_async_copy(w, wbuf.at[i], wsem.at[i])
        for i, w in enumerate((wk, wv, wq, wc, wi, wb))
    ]
    wa_rows = wa.shape[0]
    half_rows = wa_rows // 2

    def shard(index):
        return pl.ds(pl.multiple_of(index * wa_rows, wa_rows), wa_rows)

    w_part = half_rows // W_PARTS

    def part_of(index, which, c):
        begin = index * wa_rows + which * half_rows + c * w_part
        return pl.ds(pl.multiple_of(begin, w_part), w_part)

    load_wa = pltpu.make_async_copy(wa, wfull.at[shard(t)], wsem.at[6])
    load_wo = pltpu.make_async_copy(wo, wobuf, wsem.at[7])

    def block_at(index):
        return pl.ds(pl.multiple_of(index * own, own), own)

    phase("barrier")
    barrier = pltpu.get_barrier_semaphore()

    def hello(where):
        pl.semaphore_signal(barrier, inc=1, device_id=where, device_id_type=MESH)

    for peer in (near, away, diag):
        hello({"tp": peer})
    for peer in (t, near, away, diag):
        hello({"sp": mate, "tp": peer})

    plain_up = level < levels - 2
    plain_down = has_down & (level < levels - 1)

    @pl.when(plain_up)
    def _():
        hello({"sp": s + 2})

    @pl.when(plain_down)
    def _():
        hello({"sp": s - 2})

    @pl.when(high_pair == 1)
    def _():
        for which in range(2):
            for peer in range(tp):
                hello({"sp": (cross_sp // 2) * 2 + which, "tp": peer})

    @pl.when((side == 1) & has_up)
    def _():
        hello({"sp": s + 1})

    @pl.when((side == 0) & has_down)
    def _():
        hello({"sp": s - 1})

    phase("norm")
    for read in reads:
        read.wait()
    for load in (*loads, load_wa, load_wo):
        load.start()
    x = x_ref[...].astype(jnp.float32)
    held[block_at(t), :] = (rms_scale(x) * gain_ref[...]).astype(jnp.bfloat16)
    for row, ref in ((0, kg_ref), (1, qg_ref)):
        for h in range(heads):
            for m in range(2):
                at = (h * 2 + m) * comp
                gains[row : row + 1, at : at + comp] = ref[m : m + 1, :]

    phase("barrier_wait")
    expected = 7 + as_int(plain_up) + as_int(plain_down) + 2 * tp * high_pair
    pl.semaphore_wait(barrier, expected + side * ups + (1 - side) * downs)

    phase("defs")
    part = own // CHUNKS

    def chunk_at(index, c):
        return pl.ds(pl.multiple_of(index * own + c * part, part), part)

    def far_copy(c):
        spot = held.at[chunk_at(t, c)]
        return remote(spot, spot, far_send.at[c], far_recv.at[c], {"tp": away})

    def forward(c):
        spot = held.at[chunk_at(away, c)]
        return remote(spot, spot, fwd_send.at[c], fwd_recv.at[c], {"tp": near})

    far_copies = [far_copy(c) for c in range(CHUNKS)]
    forwards = [forward(c) for c in range(CHUNKS)]
    mine = held.at[block_at(t)]
    near_copy = remote(mine, mine, near_sem.at[0], near_sem.at[1], {"tp": near})
    near_copy.start()
    for copy in far_copies:
        copy.start()
    for h in range(heads):
        lamb[0, h] = jnp.full(lamb.shape[2:], lam_ref[h], jnp.float32)
    lam_copy = remote(lamb.at[0], lamb.at[1], lam_sem.at[0], lam_sem.at[1], {"tp": near})
    lam_copy.start()

    w_near = remote(wa, wfull.at[shard(t)], w_send.at[0], w_recv.at[0], {"tp": near})
    def w_far(c):
        return remote(
            wa.at[pl.ds(pl.multiple_of(side * half_rows + c * w_part, w_part), w_part)],
            wfull.at[part_of(t, side, c)], w_send.at[1 + c], w_recv.at[1 + c], {"tp": away},
        )

    def w_side(c):
        spot = wfull.at[part_of(away, side, c)]
        return remote(spot, spot, w_send.at[3 + c], w_recv.at[3 + c], mate_id)

    def w_pass(which, kind, c):
        spot = wfull.at[part_of(away, which, c)]
        slot = 5 + 2 * kind + c
        return remote(spot, spot, w_send.at[slot], w_recv.at[slot], {"tp": near})

    def w_spread(c):
        w_far(c).wait_recv()
        w_side(c).start()
        w_pass(side, 0, c).start()

    def slot_of(lev, pair):
        return lev * 2 + pair

    def group_of(lev, pair, which):
        return (lev * 2 + pair) * 2 + which

    def side_rows(which):
        return pl.ds(pl.multiple_of(which * half, half), half)

    def up_copy(lev, pair, which):
        g = group_of(lev, pair, which)
        return remote(
            kvb.at[0, slot_of(lev, pair), side_rows(which)],
            kvb.at[aside, slot_of(lev, pair), side_rows(which)],
            up_send.at[g], kv_recv.at[aside * groups + g], up_id,
        )

    def arrived(where, lev, pair, which):
        spot = kvb.at[where, slot_of(lev, pair), side_rows(which)]
        g = group_of(lev, pair, which)
        remote(spot, spot, up_send.at[g], kv_recv.at[where * groups + g], up_id).wait_recv()

    sub = own // 2

    def part_span(base, part):
        if part is None:
            return pl.ds(pl.multiple_of(base, half), half)
        return pl.ds(pl.multiple_of(base + part * own, own), own)

    def give_copy(pair, part):
        index = 0 if part is None else 1 + part
        arrival = kv_recv.at[group_of(level, pair, side)] if part is None else x_recv.at[part]
        return remote(
            give_kv.at[pair, part_span(0, part)],
            kvb.at[0, slot_of(level, pair), part_span(side * half, part)],
            gk_send.at[index], arrival, mate_id,
        )

    def q_rows(which, pair):
        return pl.ds(pl.multiple_of(which * rows + pair * half, half), half)

    def giveq_copy(pair, part):
        index = 0 if part is None else 1 + part
        return remote(
            give_q.at[pair, part_span(0, part)],
            qb.at[0, part_span(side * rows + pair * half, part)],
            gq_send.at[index], q_recv.at[index], mate_id,
        )

    def swap_q(which, pair):
        index = which * 2 + pair
        return remote(
            qb.at[0, q_rows(which, pair)], qb.at[1, q_rows(which, pair)],
            qs_send.at[index], qs_recv.at[index], cross_id,
        )

    def pass_q(which, pair):
        @pl.when(swaps)
        def _():
            swap_q(which, pair).start()

    def split(values):
        low, high = values[:, :head_cols], values[:, head_cols:]
        return jnp.where(side == 0, low, high), jnp.where(side == 0, high, low)

    def pair_rows(pair):
        return pl.ds(pl.multiple_of(pair * half, half), half)

    def scaled(block, i, gain_row, factor):
        res = jnp.dot(block, wbuf[i], preferred_element_type=jnp.float32).astype(jnp.bfloat16)
        wide = res.astype(jnp.float32)
        return (wide * group_scale(wide, comp) * (gains[gain_row : gain_row + 1] * factor)).astype(
            jnp.bfloat16
        )

    def source(pair, part):
        if part is None:
            return held[pair_rows(pair)]
        return jnp.concatenate(
            [
                held[pl.ds(pl.multiple_of(pair * half + b * own + part * sub, sub), sub)]
                for b in range(2)
            ],
            axis=0,
        )

    def place_kv(block, pair, part):
        slot = slot_of(level, pair)
        for i in range(2):
            if i == 0:
                res = scaled(block, 0, 0, 1.0)
            else:
                res = jnp.dot(block, wbuf[1], preferred_element_type=jnp.float32).astype(
                    jnp.bfloat16
                )
            keep, give = split(res)
            cols = slice(i * head_cols, (i + 1) * head_cols)
            kvb[0, slot, part_span(side * half, part), cols] = keep
            give_kv[pair, part_span(0, part), cols] = give

    def project_kv(pair, part):
        place_kv(source(pair, part), pair, part)
        send_kv(pair, part)

    def send_kv(pair, part):
        give_copy(pair, part).start()
        if part != 0:
            @pl.when(sends_own)
            def _():
                up_copy(level, pair, side).start()

    def project_q(pair, part=None):
        block = source(pair, part)
        keep, give = split(scaled(block, 2, 1, comp ** (-0.5)))
        qb[0, part_span(side * rows + pair * half, part)] = keep
        give_q[pair, part_span(0, part)] = give
        giveq_copy(pair, part).start()
        if part != 0:
            pass_q(side, pair)

    def project_conv(pair, part=None):
        block = source(pair, part)
        for i in range(3):
            res = jnp.dot(block, wbuf[3 + i], preferred_element_type=jnp.float32).astype(
                jnp.bfloat16
            )
            cols = slice(i * channels, (i + 1) * channels)
            if part is None:
                cbuf[pair_rows(pair), cols] = res
            else:
                for b in range(2):
                    begin = pl.multiple_of(pair * half + b * own + part * sub, sub)
                    cbuf[pl.ds(begin, sub), cols] = res[b * sub : (b + 1) * sub]

    def await_mate(pair, parts):
        if parts is None:
            arrived(0, level, pair, 1 - side)
        else:
            for part in parts:
                give_copy(pair, part).wait_recv()

        @pl.when(sends_own)
        def _():
            up_copy(level, pair, 1 - side).start()

    def relay(j, pair, sides=(side, 1 - side)):
        for which in sides:
            arrived(0, level - j, pair, which)
            up_copy(level - j, pair, which).start()

    queries = 2 * rows
    tile = min(TILE, half)

    def prepare(phase_index, pair):
        for which in range(2):
            @pl.when(swaps)
            def _():
                swap_q(which, pair).wait_recv()

            lane = lax.broadcasted_iota(jnp.int32, (half, both), 1)
            for h in range(per):
                q = qb[swapped, q_rows(which, pair), h * both : (h + 1) * both]
                zero = jnp.zeros_like(q)
                at = phase_index * rows + which * half
                qpad[h, at : at + half] = jnp.where(lane < comp, q, zero)
                qpad[h, queries + at : queries + at + half] = jnp.where(lane < comp, zero, q)

    def position(index):
        low = index % own
        return low // sub * own + index // own * sub + low % sub

    def run_tiles(work):
        def score(item):
            h, keys, values, at, mask = item
            return lax.dot_general(
                keys(), qpad[h, at], (((1,), (1,)), ((), ())), preferred_element_type=jnp.float32
            )

        def finish(item):
            h, values, at, p, factor = item
            acc[h, :, at] = acc[h, :, at] * factor + jnp.dot(
                values(), p, preferred_element_type=jnp.float32
            )

        ahead = [score(item) for item in work[:DEPTH]]
        late = None
        for index, (h, keys, values, at, mask) in enumerate(work):
            scores = ahead.pop(0)
            if index + DEPTH < len(work):
                ahead.append(score(work[index + DEPTH]))
            if mask is not None:
                kpos = lax.broadcasted_iota(jnp.int32, scores.shape, 0)
                qpos = mask[0] + lax.broadcasted_iota(jnp.int32, scores.shape, 1)
                if mask[1]:
                    kpos, qpos = position(kpos), position(qpos)
                scores = jnp.where(kpos <= qpos, scores, -1e30)
            old = top[h : h + 1, at]
            new = jnp.maximum(old, jnp.max(scores, axis=0, keepdims=True))
            p = jnp.exp(scores - new)
            factor = jnp.exp(old - new)
            top[h : h + 1, at] = new
            total[h : h + 1, at] = total[h : h + 1, at] * factor + jnp.sum(
                p, axis=0, keepdims=True
            )
            if late is not None:
                finish(late)
            late = (h, values, at, p.astype(jnp.bfloat16), factor)
        finish(late)

    def key_part(slot, h, begin, size):
        return lambda: kvb[swapped, slot, begin : begin + size, h * both : (h + 1) * both]

    def value_part(where, h, begin, size):
        return lambda: vt[where, h, :, begin : begin + size]

    def turn_values(slot, where):
        for h in range(per):
            cols = slice(head_cols + h * vsize, head_cols + (h + 1) * vsize)
            vt[where, h] = kvb[swapped, slot, :, cols].T

    def taken(lev, pair):
        @pl.when(swaps)
        def _():
            for which in range(2):
                arrived(1, lev, pair, which)

    def absorb(j, pair, phases, take):
        lev = job_level - j
        if take:
            taken(lev, pair)
        slot = slot_of(lev, pair)
        turn_values(slot, 0)
        run_tiles(
            [
                (
                    h, key_part(slot, h, which * half, half),
                    value_part(0, h, which * half, half), slice(start, start + tile), None,
                )
                for h in range(per)
                for ph in phases
                for m in range(2)
                for start in range(
                    m * queries + ph * rows, m * queries + (ph + 1) * rows, tile
                )
                for which in range(2)
            ]
        )

    pairs = (first, second)

    def diag_work(blocks):
        work = []
        for h in range(per):
            for q_ph, q_side, k_ph, k_side in blocks:
                same = q_ph == k_ph and q_side == k_side
                slot = slot_of(job_level, pairs[k_ph])
                for m in range(2):
                    base = m * queries + q_ph * rows + q_side * half
                    for offset in range(0, half, tile):
                        size = offset + tile if same and q_ph == 0 else half
                        work.append(
                            (
                                h, key_part(slot, h, k_side * half, size),
                                value_part(1 + k_ph, h, k_side * half, size),
                                slice(base + offset, base + offset + tile),
                                (offset, q_ph == 1) if same else None,
                            )
                        )
        return work

    def diag_ready(ph):
        taken(job_level, pairs[ph])
        turn_values(slot_of(job_level, pairs[ph]), 1 + ph)

    phase("wait_kv_weights")
    loads[0].wait()
    loads[1].wait()
    place_kv(held[block_at(t)], first, odd)
    phase("wait_near")
    near_copy.wait_recv()
    phase("kv_first")
    place_kv(held[block_at(near)], first, 1 - odd)
    send_kv(first, None)
    w_near.start()
    phase("q_first")
    loads[2].wait()
    project_q(first)
    phase("conv_first")
    for load in loads[3:]:
        load.wait()
    project_conv(first)
    tail_copy = remote(
        cbuf.at[pl.ds(rows - EDGE, EDGE), pl.ds(0, 2 * channels)], tail,
        tail_sem.at[0], tail_sem.at[1], {"sp": jnp.minimum(s + 1, sp - 1)},
    )

    @pl.when((s < sp - 1) & (first == 1))
    def _():
        tail_copy.start()

    phase("mate_first")
    await_mate(first, None)
    phase("part_a")
    for c in range(CHUNKS // 2):
        far_copies[c].wait_recv()
        forwards[c].start()
    for c in range(CHUNKS // 2):
        forwards[c].wait_recv()
    project_kv(second, 0)
    project_q(second, 0)
    project_conv(second, 0)

    phase("below_first")
    @pl.when(has_down & relays)
    def _():
        relay(1, first)

    giveq_copy(first, None).wait_recv()
    pass_q(1 - side, first)
    phase("early")
    top[...] = jnp.full_like(top, -1e30)
    total[...] = jnp.zeros_like(total)
    acc[...] = jnp.zeros_like(acc)

    def early():
        prepare(0, first)
        diag_ready(0)
        run_tiles(diag_work([(0, 0, 0, 0), (0, 1, 0, 0), (0, 1, 0, 1)]))

    for c in range(CHUNKS // 2, CHUNKS - 1):
        far_copies[c].wait_recv()
        forwards[c].start()

    for c in range(W_PARTS):
        w_far(c).start()

    @pl.when(jnp.logical_not(swaps))
    def _():
        early()

    phase("far_wait")
    far_copies[CHUNKS - 1].wait_recv()
    forwards[CHUNKS - 1].start()
    for copy in forwards[CHUNKS // 2 :]:
        copy.wait_recv()
    phase("kv_second")
    project_kv(second, 1)
    phase("q_second")
    project_q(second, 1)
    phase("conv_second")
    project_conv(second, 1)

    @pl.when((s < sp - 1) & (first == 0))
    def _():
        tail_copy.start()

    phase("below_first2")

    @pl.when((level > 1) & relays)
    def _():
        relay(2, first)

    phase("early2a")

    @pl.when(swaps & relays)
    def _():
        early()

    @pl.when(jnp.logical_not(swaps) & (job_level > 0))
    def _():
        absorb(1, first, (0,), True)

    phase("mate_second")
    await_mate(second, (0, 1))

    @pl.when(swaps)
    def _():
        for part in range(2):
            giveq_copy(second, part).wait_recv()
        swap_q(1 - side, second).start()

    phase("early2")

    @pl.when(jnp.logical_not(relays))
    def _():
        early()

    @pl.when(relays)
    def _():
        @pl.loop(2 - swapped, jnp.minimum(job_level, 2) + 1)
        def _(j):
            absorb(j, first, (0,), True)

    @pl.when(jnp.logical_not(swaps))
    def _():
        for part in range(2):
            giveq_copy(second, part).wait_recv()

    @pl.when(has_down & relays)
    def _():
        relay(1, second, (side,))

    phase("w_first")
    w_spread(0)
    phase("conv")
    def product(ref):
        gate = ref[:, :channels].astype(jnp.float32)
        other = ref[:, channels : 2 * channels].astype(jnp.float32)
        return (gate * other).astype(jnp.bfloat16).astype(jnp.float32)

    padded[EDGE:] = product(cbuf)

    @pl.when(s > 0)
    def _():
        tail_copy.wait_recv()
        padded[:EDGE] = product(tail)

    @pl.when(s == 0)
    def _():
        padded[:EDGE] = jnp.zeros((EDGE, channels), jnp.float32)

    count = taps_ref.shape[0]
    conv = jnp.zeros((rows, channels), jnp.float32)
    for tap in range(count):
        begin = EDGE - count + 1 + tap
        conv = conv + taps_ref[tap : tap + 1] * padded[begin : begin + rows]
    gated = cbuf[:, 2 * channels :].astype(jnp.float32) * conv
    cvout[...] = (gated * group_scale(gated, GROUP) * cgain_ref[...]).astype(jnp.bfloat16)
    load_wo.wait()

    def partial(target):
        return jnp.dot(cvout[block_at(target), :], wobuf[...], preferred_element_type=jnp.float32)

    cross_copy = remote(cross, cross_in, cross_send, cross_recv, {"tp": near})
    fin_copy = remote(fin, fin_in, fin_send, fin_recv, {"tp": near})
    far_sum = remote(far, far_in, fs_send, fs_recv, {"tp": away})
    phase("partial")
    cross[...] = partial(diag).astype(jnp.bfloat16)
    cross_copy.start()
    fin[...] = partial(near).astype(jnp.bfloat16)
    fin_copy.start()
    out_ref[...] = partial(t)
    phase("relay_second")

    @pl.when(has_down & (is_top == 0))
    def _():
        relay(1, second, (1 - side,))

    def settle():
        toward = partial(away)
        cross_copy.wait_recv()
        far[...] = (toward + cross_in[...].astype(jnp.float32)).astype(jnp.bfloat16)
        far_sum.start()

    @pl.when(jnp.logical_not(relays))
    def _():
        settle()

    phase("q_late")
    prepare(1, second)
    phase("near1")

    @pl.when(job_level > 0)
    def _():
        @pl.when(jnp.logical_not(relays))
        def _():
            absorb(1, first, (0,), True)

        absorb(1, first, (1,), False)

    phase("toward")

    @pl.when(relays)
    def _():
        settle()

    phase("w_far")
    w_spread(1)
    @pl.when(has_down & (is_top * odd == 1))
    def _():
        relay(1, second, (1 - side,))

    phase("near_loop")

    @pl.loop(2, job_level + 1)
    def _(j):
        @pl.when((j < level) & relays)
        def _():
            relay(j + 1, first)

        @pl.when((j > 2) | jnp.logical_not(relays))
        def _():
            absorb(j, first, (0,), True)

        absorb(j, first, (1,), False)

        @pl.when((j == 2) & (level > 1) & relays)
        def _():
            relay(2, second, (side,))

    @pl.when((level > 1) & relays)
    def _():
        relay(2, second, (1 - side,))

    phase("diag")
    diag_ready(1)
    run_tiles(
        diag_work([(1, 0, 1, 0), (1, 1, 1, 0), (1, 1, 1, 1), (1, 1, 0, 0), (0, 1, 1, 0)])
    )

    @pl.when(first == 1)
    def _():
        run_tiles(diag_work([(0, 0, 1, 0), (0, 1, 1, 1)]))

    @pl.when(first == 0)
    def _():
        run_tiles(diag_work([(1, 0, 0, 0), (1, 1, 0, 1)]))

    me8 = job_tp * 2 + side

    def piece_rows(which, target):
        return pl.ds(pl.multiple_of(which * rows + target * own, own), own)

    def o_copy(which, target, index):
        return remote(
            obuf.at[piece_rows(which, target)], hin.at[me8], o_send.at[index], o_recv.at[me8],
            {"sp": job_level * 2 + which, "tp": target},
        )

    def o_wait(which, source_tp, index):
        spot = hin.at[source_tp * 2 + which]
        return remote(spot, spot, o_send.at[index], o_recv.at[source_tp * 2 + which], mate_id)

    peers = [(1 - side, diag), (1 - side, away), (side, diag), (side, away)]
    peers += [(1 - side, t), (1 - side, near), (side, near)]

    def conclude(ph):
        span = slice(ph * rows, (ph + 1) * rows)
        other = slice(queries + ph * rows, queries + (ph + 1) * rows)
        for h in range(per):
            factor = lamb[swapped, side * per + h][0:1, 0:1]
            attn = acc[h, :, span] * (1.0 / total[h : h + 1, span])
            attn = attn - factor * (acc[h, :, other] * (1.0 / total[h : h + 1, other]))
            scale = lax.rsqrt(jnp.mean(attn * attn, axis=0, keepdims=True) + eps)
            result = ((attn * scale).T * sub_ref[...]).astype(jnp.bfloat16)
            cols = slice(h * vsize, (h + 1) * vsize)
            for which in range(2):
                base = which * half
                if ph == 0:
                    obuf[q_rows(which, first), cols] = result[base : base + half]
                else:
                    for part in range(2):
                        for b in range(2):
                            begin = which * rows + second * half + b * own + part * sub
                            at = base + part * own + b * sub
                            obuf[pl.ds(pl.multiple_of(begin, sub), sub), cols] = result[
                                at : at + sub
                            ]

    def store_logs():
        for h in range(per):
            logs = top[h : h + 1] + jnp.log(total[h : h + 1])
            for m in range(2):
                ordered = []
                for which in range(2):
                    at = m * queries + which * half
                    early_part = logs[:, at : at + half]
                    late_part = jnp.concatenate(
                        [
                            logs[:, at + rows + part * own + b * sub :][:, :sub]
                            for b in range(2)
                            for part in range(2)
                        ],
                        axis=1,
                    )
                    ordered.append(
                        jnp.concatenate(
                            [
                                jnp.where(first == 0, early_part, late_part),
                                jnp.where(first == 0, late_part, early_part),
                            ],
                            axis=1,
                        )
                    )
                low, high = ordered
                lout[0, h, m : m + 1, :] = jnp.where(side == 0, low, high)
                lout[1, h, m : m + 1, :] = jnp.where(side == 0, high, low)

    phase("far_loop")

    @pl.loop(1, job_level + 1)
    def _(j):
        absorb(j, second, (1,), True)

        @pl.when((j > 1) & (j < level) & relays)
        def _():
            relay(j + 1, second)

    phase("finish1")
    lam_copy.wait_recv()
    conclude(1)
    for index in range(4):
        which, target = peers[index]
        o_copy(which, target, index).start()
    phase("far_loop0")

    @pl.loop(1, job_level + 1)
    def _(j):
        absorb(j, second, (0,), False)

    phase("w_side")
    for c in range(W_PARTS):
        w_side(c).wait_recv()
        w_pass(1 - side, 1, c).start()

    def log_copy(index):
        which = side + index - 2 * index * side
        return remote(
            lout.at[index], lin.at[index], log_send.at[index], log_recv.at[index],
            {"sp": job_level * 2 + which, "tp": job_tp},
        )

    phase("finish0")
    store_logs()
    log_copy(1).start()

    @pl.when(swaps)
    def _():
        log_copy(0).start()

    conclude(0)
    for index in range(4, 7):
        which, target = peers[index]
        o_copy(which, target, index).start()

    @pl.when(swaps)
    def _():
        o_copy(side, t, 7).start()

    @pl.when(jnp.logical_not(swaps))
    def _():
        hin[me8] = obuf[piece_rows(side, t)]
        for h in range(per):
            log_ref[side * per + h] = lout[0, h]

    phase("conv_sum")
    fin_copy.wait_recv()
    far_sum.wait_recv()
    out_ref[...] += fin_in[...].astype(jnp.float32) + far_in[...].astype(jnp.float32)
    phase("w_wait")
    load_wa.wait()
    w_near.wait_recv()
    for c in range(W_PARTS):
        w_pass(side, 0, c).wait_recv()
        w_pass(1 - side, 1, c).wait_recv()
    phase("o_wait")
    for index, (which, source) in enumerate(peers):
        o_wait(which, source, index).wait_recv()

    @pl.when(swaps)
    def _():
        o_wait(side, t, 7).wait_recv()
        log_copy(0).wait_recv()
        for h in range(per):
            log_ref[side * per + h] = lin[0, h]

    phase("last_dot")
    lhs = jnp.concatenate([hin[i] for i in range(2 * tp)], axis=1)
    strip = out_ref.shape[1] // CHUNKS
    stores = []
    for c in range(CHUNKS):
        cols = slice(c * strip, (c + 1) * strip)
        out_ref[:, cols] += jnp.dot(lhs, wfull[:, cols], preferred_element_type=jnp.float32)
        store = pltpu.make_async_copy(out_ref.at[:, cols], out_hbm.at[:, cols], wsem.at[c])
        store.start()
        stores.append(store)
    phase("log")
    log_copy(1).wait_recv()
    for h in range(per):
        log_ref[(1 - side) * per + h] = lin[1, h]
    log_store = pltpu.make_async_copy(log_ref, log_hbm, wsem.at[CHUNKS])
    log_store.start()
    stores.append(log_store)
    phase("sends")
    for store in stores:
        store.wait()
    near_copy.wait_send()
    for copy in far_copies + forwards:
        copy.wait_send()
    for pair, part in ((first, None), (second, 0), (second, 1)):
        give_copy(pair, part).wait_send()
        giveq_copy(pair, part).wait_send()
    w_near.wait_send()
    for c in range(W_PARTS):
        for copy in (w_far(c), w_side(c), w_pass(side, 0, c), w_pass(1 - side, 1, c)):
            copy.wait_send()
    for copy in (cross_copy, fin_copy, far_sum, log_copy(1), lam_copy):
        copy.wait_send()
    for index, (which, target) in enumerate(peers):
        o_copy(which, target, index).wait_send()

    @pl.when(swaps)
    def _():
        o_copy(side, t, 7).wait_send()
        log_copy(0).wait_send()
        for which in range(2):
            for pair in range(2):
                swap_q(which, pair).wait_send()

    @pl.loop(is_top * (1 - odd) * level, level + 1 - is_top * odd)
    def _(lev):
        for pair in range(2):
            for which in range(2):
                up_copy(lev, pair, which).wait_send()

    @pl.when(s < sp - 1)
    def _():
        tail_copy.wait_send()

    phase(None)


def phase(name):
    pass


def deliver(mixed_in, log_in, mixed_out, log_out, mixed_buf, log_buf, read_sem, write_sem):
    strip = mixed_buf.shape[0] // CHUNKS
    spans = [(mixed_in, mixed_buf, mixed_out, pl.ds(c * strip, strip)) for c in range(CHUNKS)]
    spans.append((log_in, log_buf, log_out, pl.ds(0, log_buf.shape[0])))
    reads, writes = [], []
    for i, (src, buf, dst, at) in enumerate(spans):
        reads.append(pltpu.make_async_copy(src.at[at], buf.at[at], read_sem.at[i]))
        writes.append(pltpu.make_async_copy(buf.at[at], dst.at[at], write_sem.at[i]))
    for read in reads:
        read.start()
    for read, write in zip(reads, writes):
        read.wait()
        write.start()
    for write in writes:
        write.wait()


def on_device(
    inputs, norm_gain, w_query, w_key, w_value, query_gain, key_gain, lambdas, sub_gain,
    w_gate_b, w_gate_c, w_conv_in, conv_taps, conv_gain, w_out_att, w_out_conv,
):
    heads = lambdas.shape[0]
    comp = query_gain.shape[1]
    vsize = sub_gain.shape[0]
    channels = conv_gain.shape[0]
    own, width = inputs.shape
    tp = lax.axis_size("tp")
    sp = lax.axis_size("sp")
    rows = own * tp
    half = rows // 2
    qcols = heads * 2 * comp
    mine = qcols // 2
    per = heads // 2
    dma = pltpu.SemaphoreType.DMA
    bf, f32 = jnp.bfloat16, jnp.float32
    weights = (w_key, w_value, w_query, w_gate_c, w_conv_in, w_gate_b, w_out_att, w_out_conv)
    groups = sp // 2 * 4
    piece = pltpu.VMEM((own, width), bf)
    any_spec = pl.BlockSpec(memory_space=pl.ANY)
    mixed, log_sums = pl.pallas_call(
        functools.partial(layer, sp, tp, comp, heads),
        out_shape=(
            jax.ShapeDtypeStruct((own, width), f32),
            jax.ShapeDtypeStruct((heads, 2, rows), f32),
        ),
        in_specs=[any_spec] * 16,
        out_specs=(any_spec, any_spec),
        scratch_shapes=[
            pltpu.VMEM(inputs.shape, inputs.dtype),
            pltpu.VMEM((1, width), f32),
            pltpu.VMEM(query_gain.shape, f32),
            pltpu.VMEM(key_gain.shape, f32),
            pltpu.SMEM(lambdas.shape, f32),
            pltpu.VMEM((1, vsize), f32),
            pltpu.VMEM(conv_taps.shape, f32),
            pltpu.VMEM((1, channels), f32),
            pltpu.VMEM((own, width), f32),
            pltpu.VMEM((heads, 2, rows), f32),
            pltpu.VMEM((rows, width), bf),
            pltpu.VMEM((6, width, qcols), bf),
            pltpu.VMEM((tp * w_out_att.shape[0], width), bf),
            pltpu.VMEM(w_out_conv.shape, bf),
            pltpu.VMEM((8, qcols), f32),
            pltpu.VMEM((2, sp, 2 * half, 2 * mine), bf),
            pltpu.VMEM((3, per, vsize, 2 * half), bf),
            pltpu.VMEM((2, 2 * rows, mine), bf),
            pltpu.VMEM((2, half, 2 * mine), bf),
            pltpu.VMEM((2, half, mine), bf),
            pltpu.VMEM((per, 4 * rows, 2 * comp), bf),
            pltpu.VMEM((per, 4 * rows), f32),
            pltpu.VMEM((per, 4 * rows), f32),
            pltpu.VMEM((per, vsize, 4 * rows), f32),
            pltpu.VMEM((rows, 3 * channels), bf),
            pltpu.VMEM((EDGE, 2 * channels), bf),
            pltpu.VMEM((EDGE + rows, channels), f32),
            pltpu.VMEM((rows, channels), bf),
            pltpu.VMEM((2, heads, 8, 128), f32),
            piece, piece, piece, piece, piece, piece,
            pltpu.VMEM((2 * rows, per * vsize), bf),
            pltpu.VMEM((2 * tp, own, per * vsize), bf),
            pltpu.VMEM((2, per, 2, rows), f32),
            pltpu.VMEM((2, per, 2, rows), f32),
            dma((8,)), dma((2,)), dma((CHUNKS,)), dma((CHUNKS,)), dma((CHUNKS,)), dma((CHUNKS,)),
            dma((groups,)), dma((2 * groups,)), dma((3,)), dma((3,)), dma((3,)), dma((2,)),
            dma((2,)),
            dma((9,)), dma((9,)), dma(()), dma(()), dma(()), dma(()), dma(()), dma(()),
            dma((8,)), dma((2 * tp,)), dma((2,)), dma((2,)), dma((2,)),
            dma((4,)), dma((4,)),
        ],
        compiler_params=pltpu.CompilerParams(
            collective_id=0, has_side_effects=True, vmem_limit_bytes=VMEM_LIMIT
        ),
        name="layer",
    )(
        inputs, norm_gain[None], query_gain, key_gain, lambdas, sub_gain[None], conv_taps,
        conv_gain[None], *weights,
    )
    return pl.pallas_call(
        deliver,
        out_shape=(
            jax.ShapeDtypeStruct(mixed.shape, f32),
            jax.ShapeDtypeStruct(log_sums.shape, f32),
        ),
        in_specs=[any_spec, any_spec],
        out_specs=(any_spec, any_spec),
        scratch_shapes=[
            pltpu.VMEM(mixed.shape, f32),
            pltpu.VMEM(log_sums.shape, f32),
            dma((CHUNKS + 1,)),
            dma((CHUNKS + 1,)),
        ],
        compiler_params=pltpu.CompilerParams(vmem_limit_bytes=VMEM_LIMIT),
        name="deliver",
    )(mixed, log_sums)


def solution(mesh):
    in_specs = (
        P(("sp", "tp"), None),
        P(),
        P(None, "tp"),
        P(None, "tp"),
        P(None, "tp"),
        P(),
        P(),
        P("tp"),
        P(),
        P(None, "tp"),
        P(None, "tp"),
        P(None, "tp"),
        P(None, "tp"),
        P("tp"),
        P("tp", None),
        P("tp", None),
    )
    out_specs = (P(("sp", "tp"), None), P("tp", None, "sp"))
    return jax.shard_map(
        on_device, mesh=mesh, in_specs=in_specs, out_specs=out_specs, check_vma=False
    )
```
